256 devices in a mesh: ep: 64 (over z, y, core), tp: 4 (over x).
Axes of the slice: x: 4, y: 4, z: 8, core: 2. Of those that a mesh axis runs over, the one named last changes fastest.
Arguments:
- c_gate: bfloat16 [16384, 1024], P('ep', 'tp'), may hold values from -6 to 6
- b_gate: bfloat16 [16384, 1024], P('ep', 'tp'), may hold values from -6 to 6
- values: bfloat16 [16384, 1024], P('ep', 'tp'), may hold values from -6 to 6
- conv_taps: float32 [3, 1024], P(None, 'tp'), may hold values from -3.5 to 3.5
- w_mix_out: bfloat16 [1024, 2048], P('tp'), may hold values from -0.1875 to 0.1875
- moe_in: bfloat16 [32768, 2048], P(('ep', 'tp')), may hold values from -6 to 6
- norm_gain: float32 [2048], replicated, may hold values from 0.1 to 1.9
- route_ids: int32 [32768, 2], P(('ep', 'tp')), may hold values from 0 to 63, all different within a row; in each aligned block of 128 rows (0 to 127, 128 to 255, ...) at most 5 rows name the same one
- route_weights: float32 [32768, 2], P(('ep', 'tp')), may hold values from 0.1 to 1
- w_gate: bfloat16 [64, 2048, 3584], P('ep', None, 'tp'), may hold values from -0.125 to 0.125
- w_up: bfloat16 [64, 2048, 3584], P('ep', None, 'tp'), may hold values from -0.125 to 0.125
- w_down: bfloat16 [64, 3584, 2048], P('ep', 'tp'), may hold values from -0.09375 to 0.09375
Outputs:
- mixer_out: bfloat16 [16384, 2048], P(('ep', 'tp'))
- moe_out: bfloat16 [32768, 2048], P(('ep', 'tp'))
The draws below stay inside these ranges and needn't reach their ends.
Inputs may be any that keep to these rules, and one draw needn't show every extreme that they name: `route_ids`: each row names 2 different experts; in each aligned block of 128 rows (the rows of one device) no expert is named by more than 5 rows, and in every draw some expert is named by exactly 5 rows in some block.
All inputs are finite; a program needn't handle non-finite values.
Results may differ from the reference program's by a relative error of at most 0.012.
Values may be sent and summed in bfloat16 or wider, within the bound.
A program may use at most 128 MiB of HBM per device.

```python
import math
import jax
import jax.numpy as jnp
import numpy as np
from jax import lax

D = 2048
WC = 1024
FF = 3584
KCONV = 3
TOP = 2
ROWS_B = 128
EXPERTS = 64
TOKA = 16384
TOKB = 32768
CAP = 5
SLOTS = 1280
N_EP = 64
N_TP = 4


def shard_levels(stream_key, shape, shards, smallest, largest):
    factor_of, own = 1.0, jax.random.fold_in(stream_key, 6)
    for axis_at, shards_of in shards:
        draws = jnp.exp(jax.random.uniform(jax.random.fold_in(own, axis_at), (shards_of,), jnp.float32, smallest / len(shards), largest / len(shards)))
        factor_of = factor_of * jnp.repeat(draws, shape[axis_at] // shards_of).reshape([-1 if axis == axis_at else 1 for axis in range(len(shape))])
    return factor_of


def shared_out(stream_key, own, number, rows, number_of, top, limit, lean):
    ranking = jax.random.permutation(stream_key, number_of)
    crowded, ordinary = shares(number_of, rows * top, limit, lean, True), shares(number_of, rows * top, limit, lean, False)
    places = jnp.arange(number_of)

    def named(lengths, offset_by):
        used = int((lengths > 0).sum())
        fixed = max(1, used // 4)
        passed = fixed + (places - fixed + offset_by * (used - fixed)) % max(1, number_of - fixed)
        return jnp.zeros((number_of,), jnp.int32).at[ranking[jnp.where(places < fixed, places, passed)]].set(jnp.asarray(lengths, jnp.int32))

    lengths = jnp.where(number % 4 == 0, named(crowded, number // 4), named(ordinary, number - number // 4 - 1))
    mixed = jax.random.permutation(jax.random.fold_in(own, 3), number_of)
    giver, sink = mixed[0:number_of // 2 * 2:2], mixed[1:number_of // 2 * 2:2]
    margin = jnp.minimum(lengths[giver] - 1, limit - lengths[sink]) // 2
    margin = jnp.where((giver == ranking[0]) | (sink == ranking[0]) | (lengths[sink] == 0), 0, jnp.maximum(margin, 0))
    passed = jax.random.randint(jax.random.fold_in(own, 4), (number_of // 2,), 0, 1 << 20) % (margin + 1)
    lengths = lengths.at[giver].add(-passed).at[sink].add(passed)
    labels = jnp.searchsorted(jnp.cumsum(lengths), jnp.arange(rows * top), side="right").astype(jnp.int32)
    grid = labels.reshape(top, rows).T
    grid = grid[jax.random.permutation(jax.random.fold_in(own, 1), rows)]
    offset_by = jax.random.randint(jax.random.fold_in(own, 2), (rows, 1), 0, top)
    return jnp.take_along_axis(grid, (jnp.arange(top)[None, :] + offset_by) % top, axis=1)


def shares(number_of, total, most, skew, full):
    weights = [(1 << 20) // math.isqrt(grade ** skew) + 1 for grade in range(1, number_of + 1)]
    largest = most if full else min(most, max(-(-total // number_of), total * weights[0] // sum(weights)))
    least = 1 if total - largest >= number_of - 1 else 0
    holding, rest = [largest] + [least] * (number_of - 1), total - largest - least * (number_of - 1)
    while rest > 0:
        candidates = [i for i in range(1, number_of) if holding[i] < largest] or [i for i in range(1, number_of) if holding[i] < most]
        pool, remaining = sum([weights[i] for i in candidates]), rest
        for i in candidates:
            extra = min(most - holding[i], max(1, remaining * weights[i] // pool), rest)
            holding[i] = holding[i] + extra
            rest = rest - extra
    return np.array(holding)


def gaussian(stream_key, shape, deviation, limit, split=(), kind=jnp.bfloat16):
    drawn = deviation * jax.random.normal(stream_key, shape, jnp.float32)
    if split:
        drawn = drawn * shard_levels(stream_key, shape, split, -0.22, 0.18)
    return jnp.clip(drawn, -limit, limit).astype(kind)


def setup_inputs(seed: int = 0) -> dict:
    streams_of = jax.random.split(jax.random.key(seed), 13)
    c_gate = gaussian(streams_of[0], (TOKA, WC), 1.0, 6.0, ((0, 64), (1, 4)))
    b_gate = gaussian(streams_of[1], (TOKA, WC), 1.0, 6.0, ((0, 64), (1, 4)))
    values = gaussian(streams_of[2], (TOKA, WC), 1.0, 6.0, ((0, 64), (1, 4)))
    conv_taps = gaussian(streams_of[3], (KCONV, WC), KCONV ** -0.5, 3.5, ((1, 4),), jnp.float32)
    w_mix_out = gaussian(streams_of[4], (WC, D), WC ** -0.5, 0.1875, ((0, 4),))
    moe_in = gaussian(streams_of[5], (TOKB, D), 1.0, 6.0, ((0, 256),))
    norm_gain = jnp.clip(1.0 + 0.18 * jax.random.normal(streams_of[6], (D,), jnp.float32), 0.1, 1.9)
    route_ids_keys = jax.random.split(jax.random.fold_in(streams_of[7], 1), TOKB // ROWS_B)
    route_ids_turns = jax.random.permutation(jax.random.fold_in(streams_of[7], 3), TOKB // ROWS_B)
    route_ids = jax.vmap(lambda own, number: shared_out(jax.random.fold_in(streams_of[7], 2), own, number, ROWS_B, EXPERTS, TOP, CAP, 1))(route_ids_keys, route_ids_turns).reshape((TOKB, TOP))
    route_weights = jnp.clip(0.1 + 0.9 * jax.random.uniform(streams_of[8], (TOKB, TOP), jnp.float32) ** shard_levels(streams_of[8], (TOKB, TOP), ((0, 256),), -0.2, 0.2), 0.1, 1.0)
    w_gate = gaussian(streams_of[9], (EXPERTS, D, FF), D ** -0.5, 0.125, ((0, 64), (2, 4)))
    w_up = gaussian(streams_of[10], (EXPERTS, D, FF), D ** -0.5, 0.125, ((0, 64), (2, 4)))
    w_down = gaussian(streams_of[11], (EXPERTS, FF, D), FF ** -0.5, 0.09375, ((0, 64), (1, 4)))
    return {"c_gate": c_gate, "b_gate": b_gate, "values": values, "conv_taps": conv_taps, "w_mix_out": w_mix_out, "moe_in": moe_in, "norm_gain": norm_gain, "route_ids": route_ids, "route_weights": route_weights, "w_gate": w_gate, "w_up": w_up, "w_down": w_down}


EPS = 1e-06

def grouped_product(left, right, groups):
    rows = left.shape[0]
    width = left.shape[1] // groups
    left_groups = left.reshape(rows, groups, width)
    right_groups = right.reshape(groups, width, right.shape[1])
    total = jnp.zeros((rows, right.shape[1]), jnp.float32)
    for group in range(groups):
        partial_value = jnp.dot(left_groups[:, group], right_groups[group], preferred_element_type=jnp.float32).astype(jnp.bfloat16)
        partial_value = lax.optimization_barrier(partial_value)
        total = total + partial_value.astype(jnp.float32)
    return total.astype(jnp.bfloat16)

def reference(c_gate, b_gate, values, conv_taps, w_mix_out, moe_in, norm_gain, route_ids, route_weights, w_gate, w_up, w_down):
    product = c_gate.astype(jnp.float32) * values.astype(jnp.float32)
    extended = jnp.concatenate([jnp.zeros((KCONV - 1, WC), jnp.float32), product], 0)
    convolved = jnp.zeros((TOKA, WC), jnp.float32)
    for offset in range(KCONV):
        convolved = convolved + conv_taps[offset][None, :] * extended[offset:offset + TOKA]
    mixed = (b_gate.astype(jnp.float32) * convolved).astype(jnp.bfloat16)
    mixer_out = grouped_product(mixed, w_mix_out, N_TP)
    stream = moe_in.astype(jnp.float32)
    scale = lax.rsqrt(lax.optimization_barrier(jnp.mean(stream * stream, axis=1, keepdims=True)) + EPS)
    normed = (stream * scale * norm_gain[None, :]).astype(jnp.bfloat16)
    copies = TOKB * TOP
    sources = N_EP * N_TP
    flat_ids = route_ids.reshape(sources, ROWS_B * TOP)
    onehot = (flat_ids[:, :, None] == jnp.arange(EXPERTS, dtype=jnp.int32)[None, None, :]).astype(jnp.int32)
    before = jnp.cumsum(onehot, axis=1) - onehot
    ranks_in = lax.optimization_barrier(jnp.sum(before * onehot, axis=2))
    slot_of = jnp.arange(sources, dtype=jnp.int32)[:, None] * CAP + ranks_in
    table = jnp.full((EXPERTS, SLOTS), copies, jnp.int32)
    table = table.at[flat_ids.reshape(-1), slot_of.reshape(-1)].set(jnp.arange(copies, dtype=jnp.int32))
    padded_rows = jnp.concatenate([normed, jnp.zeros((1, D), jnp.bfloat16)], 0)
    padded_weights = jnp.concatenate([route_weights.reshape(-1), jnp.zeros((1,), jnp.float32)], 0)

    def per_expert(carry, inputs):
        expert_table, gate_mat, up_mat, down_mat = inputs
        row_index = expert_table // TOP
        rows = padded_rows[row_index]
        gate_val = jnp.dot(rows, gate_mat, preferred_element_type=jnp.float32)
        up_val = jnp.dot(rows, up_mat, preferred_element_type=jnp.float32)
        hidden = (jax.nn.silu(gate_val) * up_val).astype(jnp.bfloat16)
        expert_out = grouped_product(hidden, down_mat, N_TP)
        weighted = expert_out.astype(jnp.float32) * padded_weights[expert_table][:, None]
        carry = carry.at[row_index].add(weighted, mode='drop')
        return (carry, None)
    summed, unused = lax.scan(per_expert, jnp.zeros((TOKB, D), jnp.float32), (table, w_gate, w_up, w_down))
    moe_out = summed.astype(jnp.bfloat16)
    return (mixer_out, moe_out)
```

```python
import functools

import jax
import jax.numpy as jnp
import numpy as np
from jax import lax
from jax.experimental import pallas as pl
from jax.experimental.pallas import tpu as pltpu
from jax.sharding import PartitionSpec as P

EPS = 1e-06
MESH = pl.DeviceIdType.MESH
F32 = jnp.float32
BF16 = jnp.bfloat16
CAP = 5
PAD = 8


class Plan:
    def __init__(self, n_ep, n_tp, width, hidden, rows, tokens, channels):
        self.G = int(round(n_ep**0.5))
        self.NZ = n_ep // self.G
        assert self.G * self.NZ == n_ep and self.G == self.NZ and n_tp == 4
        self.X = n_tp
        self.D, self.F, self.T = width, hidden, rows
        self.TA, self.C = tokens, channels
        self.CB = CAP * self.G
        self.R = self.CB * self.NZ
        self.GS = 2 if self.NZ >= 8 else 1
        self.NG = self.NZ // self.GS
        self.dz = [0]
        for step in range(1, self.NZ // 2 + 1):
            self.dz.append(step)
            if step != self.NZ - step:
                self.dz.append(-step)
        assert len(self.dz) == self.NZ

    def off(self, k, rel, jj=0):
        return ((k * self.X + rel) * self.GS + jj) * self.CB


def body(
    p,
    c_gate,
    b_gate,
    values,
    conv_taps,
    w_mix_hbm,
    moe_in,
    norm_gain,
    route_ids,
    route_weights,
    perm,
    w_gate_hbm,
    w_up_hbm,
    w_down_hbm,
    mixer_out,
    moe_out,
    w_mix,
    w_gate,
    w_up,
    w_down,
    product,
    halo,
    mixed,
    m_part,
    m_turn,
    m_minus,
    m_plus,
    normed,
    send_a,
    recv_a,
    send_b,
    gathered,
    hid,
    part,
    turn,
    s_minus,
    s_plus,
    out_b,
    ret_b,
    send_r,
    ret_a,
    w_sem,
    halo_sem,
    a_sem,
    b_sem,
    ag_sem,
    fw_sem,
    rs_sem,
    mx_sem,
    rb_sem,
    ra_sem,
):
    G, NZ, X, D, F, T, CB, R, GS, NG = p.G, p.NZ, p.X, p.D, p.F, p.T, p.CB, p.R, p.GS, p.NG
    ep, x = lax.axis_index("ep"), lax.axis_index("tp")
    z, g = ep // G, ep % G
    half = D // 2

    def at(zz, gg, xx):
        return {"ep": zz * G + gg, "tp": xx}

    right, left = at(z, g, (x + 1) % X), at(z, g, (x + X - 1) % X)
    after = {"ep": (ep + 1) % (G * NZ), "tp": x}
    before = {"ep": (ep + G * NZ - 1) % (G * NZ), "tp": x}
    plane = [at(z, (g + d) % G, x) for d in range(G)]
    plane_back = [at(z, (g + G - d) % G, x) for d in range(G)]
    line = [at((z + NZ + dz) % NZ, g, x) for dz in p.dz]
    line_back = [at((z + NZ - dz) % NZ, g, x) for dz in p.dz]

    barrier = pltpu.get_barrier_semaphore()
    peers = plane[1:] + line[1:] + [right, left, after, before]
    for peer in peers:
        pl.semaphore_signal(barrier, inc=1, device_id=peer, device_id_type=MESH)

    def load(src, dst, i):
        copy = pltpu.make_async_copy(src, dst, w_sem.at[i])
        copy.start()
        return copy

    loads = [
        load(w_mix_hbm, w_mix, 0),
        load(w_gate_hbm.at[0], w_gate, 1),
        load(w_up_hbm.at[0], w_up, 2),
        load(w_down_hbm.at[0], w_down, 3),
    ]
    pending = []

    def remote(src, dst, sems, i, peer):
        copy = pltpu.make_async_remote_copy(
            src_ref=src,
            dst_ref=dst,
            send_sem=sems.at[0, i],
            recv_sem=sems.at[1, i],
            device_id=peer,
            device_id_type=MESH,
        )
        pending.append(copy)
        return copy

    def start(*args):
        copy = remote(*args)
        copy.start()
        return copy

    tokens = p.TA
    product[8 : 8 + tokens, :] = c_gate[...].astype(F32) * values[...].astype(F32)

    stream = moe_in[...].astype(F32)
    scale = lax.rsqrt(jnp.mean(stream * stream, axis=1, keepdims=True) + EPS)
    normed[...] = (stream * scale * norm_gain[...]).astype(BF16)

    rows_i = lax.broadcasted_iota(jnp.int32, (T, T), 0)
    cols_i = lax.broadcasted_iota(jnp.int32, (T, T), 1)
    eye, earlier = rows_i == cols_i, cols_i < rows_i

    def as_row(col):
        return jnp.sum(jnp.where(eye, col.astype(F32), 0.0), axis=0, keepdims=True).astype(jnp.int32)

    ids = [route_ids[:, 0:1], route_ids[:, 1:2]]
    id_rows = [as_row(col) for col in ids]
    slots = []
    for col in ids:
        seen = jnp.zeros((T, 1), F32)
        for row in id_rows:
            seen = seen + jnp.sum(
                jnp.where(earlier & (col == row), 1.0, 0.0), axis=1, keepdims=True
            )
        rank = seen.astype(jnp.int32)
        to_g = (col & (G - 1)) - g
        to_g = jnp.where(to_g < 0, to_g + G, to_g)
        to_z = (col >> (G.bit_length() - 1)) - z
        to_z = jnp.where(to_z < 0, to_z + NZ, to_z)
        slot_z = jnp.where(
            to_z == 0, 0, jnp.where(to_z <= NZ // 2, 2 * to_z - 1, 2 * (NZ - to_z))
        )
        slots.append(to_g * CB + slot_z * CAP + rank)
    slot_rows = [as_row(col) for col in slots]
    slot_i = lax.broadcasted_iota(jnp.int32, (R, T), 0)
    pick = jnp.where((slot_i == slot_rows[0]) | (slot_i == slot_rows[1]), 1.0, 0.0).astype(BF16)
    wide = min(512, D)

    def pack(i, _):
        cols = pl.ds(pl.multiple_of(i * wide, wide), wide)
        packed = jnp.dot(pick, normed[:, cols], preferred_element_type=F32).astype(BF16)
        send_a[0:R, cols] = packed
        recv_a[0:CB, cols] = packed[0:CB]
        return 0

    lax.fori_loop(0, D // wide, pack, 0)

    pl.semaphore_wait(barrier, len(peers))

    halo_copy = start(product.at[pl.ds(tokens, 8)], halo, halo_sem, 0, after)
    a_copies = [
        start(send_a.at[pl.ds(d * CB, CB)], recv_a.at[pl.ds(d * CB, CB)], a_sem, d, plane[d])
        for d in range(1, G)
    ]

    def rs_start(src, rows, offs, dst_off, turn, minus, plus, c0, c1, sems, i):
        mid = (c0 + c1) // 2
        lo, hi = pl.ds(c0, mid - c0), pl.ds(mid, c1 - mid)
        o0, o1, o2, o3 = (pl.ds(o, rows) for o in offs)
        od = pl.ds(dst_off, rows)
        c = {}
        c["tl"] = start(src.at[o2, lo], turn.at[od, lo], sems, i, right)
        c["tr"] = start(src.at[o2, hi], turn.at[od, hi], sems, i + 1, left)
        c["mh"] = start(src.at[o1, hi], minus.at[od, hi], sems, i + 2, right)
        c["pl"] = start(src.at[o3, lo], plus.at[od, lo], sems, i + 3, left)

        def middle():
            c["tl"].wait_recv()
            src[o1, lo] = (src[o1, lo].astype(F32) + turn[od, lo].astype(F32)).astype(BF16)
            c["ml"] = start(src.at[o1, lo], minus.at[od, lo], sems, i + 4, right)
            c["tr"].wait_recv()
            src[o3, hi] = (src[o3, hi].astype(F32) + turn[od, hi].astype(F32)).astype(BF16)
            c["ph"] = start(src.at[o3, hi], plus.at[od, hi], sems, i + 5, left)

        def end():
            for name in ("mh", "pl", "ml", "ph"):
                c[name].wait_recv()
            cols = pl.ds(c0, c1 - c0)
            total = src[o0, cols].astype(F32) + minus[od, cols].astype(F32)
            return (total + plus[od, cols].astype(F32)).astype(BF16)

        return middle, end

    halo_copy.wait_recv()
    product[0:8, :] = jnp.where(ep == 0, 0.0, halo[...])
    convolved = jnp.zeros((tokens, p.C), F32)
    taps = conv_taps.shape[0]
    for k in range(taps):
        convolved = convolved + conv_taps[k : k + 1, :] * product[pl.ds(8 - taps + 1 + k, tokens), :]
    mixed[...] = (b_gate[...].astype(F32) * convolved).astype(BF16)
    loads[0].wait()
    m_rows = tokens // X
    for rel in range(X):
        own = pl.ds(pl.multiple_of(((x + rel) % X) * m_rows, m_rows), m_rows)
        m_part[pl.ds(rel * m_rows, m_rows), :] = jnp.dot(
            mixed[own, :], w_mix[...], preferred_element_type=F32
        ).astype(BF16)
    m_middle, m_end = rs_start(
        m_part, m_rows, [rel * m_rows for rel in range(X)], 0, m_turn, m_minus, m_plus, 0, D, mx_sem, 0
    )

    for copy in a_copies:
        copy.wait_recv()

    def turn_in(i, _):
        cols = pl.ds(pl.multiple_of(i * wide, wide), wide)
        moved = jnp.dot(perm[...], recv_a[0:R, cols], preferred_element_type=F32).astype(BF16)
        send_b[0:R, cols] = moved
        gathered[0:CB, cols] = moved[0:CB]
        return 0

    lax.fori_loop(0, D // wide, turn_in, 0)

    def where(j, rel):
        return pl.ds(p.off(j // GS, rel, j % GS), CB)

    b_copies = [None] + [
        start(send_b.at[pl.ds(j * CB, CB)], gathered.at[where(j, 0)], b_sem, j, line[j])
        for j in range(1, NZ)
    ]
    ag, fw = {}, {}

    def gather_out(j):
        if j:
            b_copies[j].wait_recv()
        ag[j] = (
            start(gathered.at[where(j, 0)], gathered.at[where(j, 3)], ag_sem, 2 * j, right),
            start(gathered.at[where(j, 0)], gathered.at[where(j, 1)], ag_sem, 2 * j + 1, left),
        )

    def gather_on(j):
        lo, hi = pl.ds(0, half), pl.ds(half, half)
        ag[j][0].wait_recv()
        to_right = start(gathered.at[where(j, 3), lo], gathered.at[where(j, 2), lo], fw_sem, 2 * j, right)
        ag[j][1].wait_recv()
        to_left = start(gathered.at[where(j, 1), hi], gathered.at[where(j, 2), hi], fw_sem, 2 * j + 1, left)
        fw[j] = (to_right, to_left)

    rows_k = X * GS * CB

    def compute(k):
        for j in range(k * GS, (k + 1) * GS):
            fw[j][0].wait_recv()
            fw[j][1].wait_recv()
        r0 = p.off(k, 0)

        def up(t, _):
            cols = pl.ds(pl.multiple_of(t * 128, 128), 128)
            pair = jnp.concatenate([w_gate[:, cols], w_up[:, cols]], axis=1)
            both = jnp.dot(gathered[r0 : r0 + rows_k, :], pair, preferred_element_type=F32)
            hid[:, cols] = (jax.nn.silu(both[:, :128]) * both[:, 128:]).astype(BF16)
            return 0

        lax.fori_loop(0, F // 128, up, 0)

        def down(n, _):
            cols = pl.ds(pl.multiple_of(n * wide, wide), wide)
            part[r0 : r0 + rows_k, cols] = jnp.dot(
                hid[...], w_down[:, cols], preferred_element_type=F32
            ).astype(BF16)
            return 0

        lax.fori_loop(0, D // wide, down, 0)

    rs = {}
    rb = {}

    def sum_start(k):
        rs[k] = rs_start(
            part, GS * CB, [p.off(k, rel) for rel in range(X)], k * GS * CB,
            turn, s_minus, s_plus, 0, D, rs_sem, 6 * k,
        )

    def sum_end(k):
        total = rs[k][1]()
        for jj in range(GS):
            j = k * GS + jj
            rows = pl.ds(j * CB, CB)
            block = total[jj * CB : (jj + 1) * CB]
            if j == 0:
                ret_b[rows, :] = block
            else:
                out_b[rows, :] = block
                rb[j] = start(out_b.at[rows], ret_b.at[rows], rb_sem, j, line_back[j])

    m_middle()
    for s in range(NZ):
        gather_out(s)
        if s >= 1:
            gather_on(s - 1)
        if s == GS:
            for copy in loads[1:]:
                copy.wait()
        if s > GS and (s - 1) % GS == 0:
            compute((s - 1) // GS - 1)
        if s == NZ - 1:
            mixer_out[...] = m_end()
    gather_on(NZ - 1)
    order = list(range(NG // 2, NG)) + list(range(NG // 2 - 1, -1, -1))
    sum_start(order[0])
    compute(NG - 1)
    for i in range(NG + 1):
        if i + 1 < NG:
            sum_start(order[i + 1])
        if i < NG:
            rs[order[i]][0]()
        if i >= 1:
            sum_end(order[i - 1])

    for j in range(1, NZ):
        rb[j].wait_recv()

    def turn_out(i, _):
        cols = pl.ds(pl.multiple_of(i * wide, wide), wide)
        moved = jnp.dot(perm[...], ret_b[0:R, cols], preferred_element_type=F32).astype(BF16)
        send_r[0:R, cols] = moved
        ret_a[0:CB, cols] = moved[0:CB]
        return 0

    lax.fori_loop(0, D // wide, turn_out, 0)
    ra = [
        start(send_r.at[pl.ds(d * CB, CB)], ret_a.at[pl.ds(d * CB, CB)], ra_sem, d, plane_back[d])
        for d in range(1, G)
    ]
    slot_j = lax.broadcasted_iota(jnp.int32, (T, R), 1)
    mix = jnp.where(slot_j == slots[0], route_weights[:, 0:1], 0.0)
    mix = mix + jnp.where(slot_j == slots[1], route_weights[:, 1:2], 0.0)
    mix_hi = mix.astype(BF16)
    mix_lo = (mix - mix_hi.astype(F32)).astype(BF16)
    for copy in ra:
        copy.wait_recv()

    def combine(i, _):
        cols = pl.ds(pl.multiple_of(i * wide, wide), wide)
        rows = ret_a[0:R, cols]
        total = jnp.dot(mix_hi, rows, preferred_element_type=F32)
        total = total + jnp.dot(mix_lo, rows, preferred_element_type=F32)
        moe_out[:, cols] = total.astype(BF16)
        return 0

    lax.fori_loop(0, D // wide, combine, 0)
    for copy in pending:
        copy.wait_send()


def permutation(p):
    matrix = np.zeros((p.R, p.R), np.float32)
    for j in range(p.NZ):
        for d in range(p.G):
            for r in range(CAP):
                matrix[j * p.CB + d * CAP + r, d * p.CB + j * CAP + r] = 1.0
    return jnp.asarray(matrix, BF16)


def on_device(
    c_gate, b_gate, values, conv_taps, w_mix_out, moe_in, norm_gain,
    route_ids, route_weights, w_gate, w_up, w_down,
):
    n_ep, n_tp = lax.axis_size("ep"), lax.axis_size("tp")
    p = Plan(n_ep, n_tp, moe_in.shape[1], w_gate.shape[2], moe_in.shape[0], *c_gate.shape)
    D, F, T, R, CB, G, NZ, X = p.D, p.F, p.T, p.R, p.CB, p.G, p.NZ, p.X
    m_rows = p.TA // X
    vmem = pl.BlockSpec(memory_space=pltpu.VMEM)
    hbm = pl.BlockSpec(memory_space=pl.ANY)
    block = pltpu.VMEM((R + PAD, D), BF16)
    dma = pltpu.SemaphoreType.DMA
    return pl.pallas_call(
        functools.partial(body, p),
        name="mixer_and_experts",
        out_shape=(
            jax.ShapeDtypeStruct((m_rows, D), BF16),
            jax.ShapeDtypeStruct((T, D), BF16),
        ),
        in_specs=[vmem, vmem, vmem, vmem, hbm, vmem, vmem, vmem, vmem, vmem, hbm, hbm, hbm],
        out_specs=(vmem, vmem),
        scratch_shapes=[
            pltpu.VMEM(w_mix_out.shape, BF16),
            pltpu.VMEM((D, F), BF16),
            pltpu.VMEM((D, F), BF16),
            pltpu.VMEM((F, D), BF16),
            pltpu.VMEM((p.TA + 8, p.C), F32),
            pltpu.VMEM((8, p.C), F32),
            pltpu.VMEM((p.TA, p.C), BF16),
            pltpu.VMEM((p.TA, D), BF16),
            pltpu.VMEM((m_rows, D), BF16),
            pltpu.VMEM((m_rows, D), BF16),
            pltpu.VMEM((m_rows, D), BF16),
            pltpu.VMEM((T, D), BF16),
            block,
            block,
            block,
            pltpu.VMEM((X * R + PAD, D), BF16),
            pltpu.VMEM((X * p.GS * CB, F), BF16),
            pltpu.VMEM((X * R + PAD, D), BF16),
            block,
            block,
            block,
            block,
            block,
            block,
            block,
            dma((4,)),
            dma((2, 1)),
            dma((2, G)),
            dma((2, NZ)),
            dma((2, 2 * NZ)),
            dma((2, 2 * NZ)),
            dma((2, 6 * p.NG)),
            dma((2, 6)),
            dma((2, NZ)),
            dma((2, G)),
        ],
        compiler_params=pltpu.CompilerParams(
            collective_id=0, has_side_effects=True, vmem_limit_bytes=60 * 2**20
        ),
    )(
        c_gate, b_gate, values, conv_taps, w_mix_out, moe_in, norm_gain.reshape(1, -1),
        route_ids, route_weights, permutation(p), w_gate, w_up, w_down,
    )


def solution(mesh):
    return jax.shard_map(
        on_device,
        mesh=mesh,
        in_specs=(
            P("ep", "tp"),
            P("ep", "tp"),
            P("ep", "tp"),
            P(None, "tp"),
            P("tp", None),
            P(("ep", "tp"), None),
            P(),
            P(("ep", "tp"), None),
            P(("ep", "tp"), None),
            P("ep", None, "tp"),
            P("ep", None, "tp"),
            P("ep", "tp", None),
        ),
        out_specs=(P(("ep", "tp"), None), P(("ep", "tp"), None)),
        check_vma=False,
    )
```

```python
import functools
import itertools

import jax
import jax.numpy as jnp
import numpy as np
from jax import lax
from jax.experimental import pallas as pl
from jax.experimental.pallas import tpu as pltpu
from jax.sharding import PartitionSpec as P

EPS = 1e-06
MESH = pl.DeviceIdType.MESH
F32 = jnp.float32
BF16 = jnp.bfloat16
CAP = 5
PAD = 8


class Plan:
    def __init__(self, n_ep, n_tp, width, hidden, rows, tokens, channels):
        self.G = int(round(n_ep**0.5))
        self.NZ = n_ep // self.G
        assert self.G * self.NZ == n_ep and self.G == self.NZ and n_tp == 4
        self.X = n_tp
        self.D, self.F, self.T = width, hidden, rows
        self.TA, self.C = tokens, channels
        self.CB = CAP * self.G
        self.R = self.CB * self.NZ
        self.GS = 2
        self.NG = self.NZ // self.GS
        far = self.NZ // 2
        self.dz = [0]
        for step in range(1, far - 1):
            self.dz += [-step, step]
        self.dz += [far, 1 - far, far - 1]
        assert len(self.dz) == self.NZ
        self.by_distance = sorted(range(self.NZ), key=lambda j: abs(self.dz[j]))
        eighth = width // 8
        self.QA = spans([3 * eighth, 5 * eighth])
        self.QR = spans([3 * eighth, 2 * eighth, 2 * eighth, eighth])

    def off(self, k, rel, jj=0):
        return ((k * self.X + rel) * self.GS + jj) * self.CB


def spans(widths):
    ends = list(itertools.accumulate(widths))
    return [(end - width, end) for width, end in zip(widths, ends)]


def scoped(name, f, *a):
    with jax.named_scope(name):
        return f(*a)


def body(
    p,
    c_gate,
    b_gate,
    values,
    conv_taps,
    w_mix_hbm,
    moe_in,
    norm_gain,
    route_ids,
    route_weights,
    perm,
    w_gate_hbm,
    w_up_hbm,
    w_down_hbm,
    mixer_out,
    moe_out,
    w_mix,
    w_gate,
    w_up,
    w_down,
    product,
    halo,
    mixed,
    m_part,
    m_turn,
    m_minus,
    m_plus,
    normed,
    send_a,
    recv_a,
    send_b,
    gathered,
    hid,
    part,
    turn,
    s_minus,
    s_plus,
    out_b,
    ret_b,
    send_r,
    ret_a,
    mix_hi,
    mix_lo,
    w_sem,
    send_sem,
    halo_sem,
    a_sem,
    b_sem,
    ag_sem,
    fw_sem,
    rs_sem,
    mx_sem,
    rb_sem,
    ra_sem,
):
    G, NZ, X, D, F, T, CB, R, GS, NG = p.G, p.NZ, p.X, p.D, p.F, p.T, p.CB, p.R, p.GS, p.NG
    ep, x = lax.axis_index("ep"), lax.axis_index("tp")
    z, g = ep // G, ep % G

    def at(zz, gg, xx):
        return {"ep": zz * G + gg, "tp": xx}

    right, left = at(z, g, (x + 1) % X), at(z, g, (x + X - 1) % X)
    after = {"ep": (ep + 1) % (G * NZ), "tp": x}
    before = {"ep": (ep + G * NZ - 1) % (G * NZ), "tp": x}
    plane = [at(z, (g + d) % G, x) for d in range(G)]
    plane_back = [at(z, (g + G - d) % G, x) for d in range(G)]
    line = [at((z + NZ + dz) % NZ, g, x) for dz in p.dz]
    line_back = [at((z + NZ - dz) % NZ, g, x) for dz in p.dz]

    barrier = pltpu.get_barrier_semaphore()
    peers = plane[1:] + line[1:] + [right, left, after, before]
    for peer in peers:
        pl.semaphore_signal(barrier, inc=1, device_id=peer, device_id_type=MESH)

    def load(src, dst, i):
        copy = pltpu.make_async_copy(src, dst, w_sem.at[i])
        copy.start()
        return copy

    loads = [
        load(w_mix_hbm, w_mix, 0),
        load(w_gate_hbm.at[0], w_gate, 1),
        load(w_up_hbm.at[0], w_up, 2),
        load(w_down_hbm.at[0], w_down, 3),
    ]
    def start(src, dst, send, recv, peer):
        copy = pltpu.make_async_remote_copy(
            src_ref=src,
            dst_ref=dst,
            send_sem=send_sem.at[send],
            recv_sem=recv,
            device_id=peer,
            device_id_type=MESH,
        )
        copy.start()
        return copy

    def arrived(ref, recv):
        pltpu.make_async_remote_copy(
            src_ref=ref, dst_ref=ref, send_sem=send_sem.at[0], recv_sem=recv,
            device_id=right, device_id_type=MESH,
        ).wait_recv()

    def sent(ref, send):
        pltpu.make_async_remote_copy(
            src_ref=ref, dst_ref=ref, send_sem=send_sem.at[send], recv_sem=halo_sem.at[0],
            device_id=right, device_id_type=MESH,
        ).wait_send()

    HALO, A, B, AG, FW, RS, MX, RB, RA = range(9)

    tokens = p.TA
    product[8 : 8 + tokens, :] = c_gate[...].astype(F32) * values[...].astype(F32)

    stream = moe_in[...].astype(F32)
    scale = lax.rsqrt(jnp.mean(stream * stream, axis=1, keepdims=True) + EPS)
    normed[...] = (stream * scale * norm_gain[...]).astype(BF16)

    rows_i = lax.broadcasted_iota(jnp.int32, (T, T), 0)
    cols_i = lax.broadcasted_iota(jnp.int32, (T, T), 1)
    eye, earlier = rows_i == cols_i, cols_i < rows_i

    def as_row(col):
        return jnp.sum(jnp.where(eye, col, 0.0), axis=0, keepdims=True)

    def as_col(row):
        return jnp.sum(jnp.where(eye, row, 0.0), axis=1, keepdims=True)

    id_rows = [route_ids[k : k + 1, :].astype(F32) for k in range(2)]
    slots = []
    for col in [as_col(row) for row in id_rows]:
        seen = jnp.zeros((T, 1), F32)
        for row in id_rows:
            seen = seen + jnp.sum(
                jnp.where(earlier & (col == row), 1.0, 0.0), axis=1, keepdims=True
            )
        rank, expert = seen.astype(jnp.int32), col.astype(jnp.int32)
        to_g = (expert & (G - 1)) - g
        to_g = jnp.where(to_g < 0, to_g + G, to_g)
        to_z = (expert >> (G.bit_length() - 1)) - z
        to_z = jnp.where(to_z < 0, to_z + NZ, to_z)
        slot_z = jnp.zeros_like(to_z)
        for j, dz in enumerate(p.dz):
            slot_z = jnp.where(to_z == dz % NZ, j, slot_z)
        slots.append(to_g * CB + slot_z * CAP + rank)
    slot_rows = [as_row(col.astype(F32)).astype(jnp.int32) for col in slots]
    slot_i = lax.broadcasted_iota(jnp.int32, (R, T), 0)
    pick = jnp.where((slot_i == slot_rows[0]) | (slot_i == slot_rows[1]), 1.0, 0.0).astype(BF16)
    wide = min(512, D)

    def pack(i, _):
        cols = pl.ds(pl.multiple_of(i * wide, wide), wide)
        packed = jnp.dot(pick, normed[:, cols], preferred_element_type=F32).astype(BF16)
        send_a[0:R, cols] = packed
        recv_a[0:CB, cols] = packed[0:CB]
        return 0

    scoped("pack", lambda: lax.fori_loop(0, D // wide, pack, 0))
    scoped("barrier", pl.semaphore_wait, barrier, len(peers))

    start(product.at[pl.ds(tokens, 8)], halo, HALO, halo_sem.at[0], after)

    def cols_of(span):
        return pl.ds(span[0], span[1] - span[0])

    for q, span in enumerate(p.QA):
        for d in range(1, G):
            start(
                send_a.at[pl.ds(d * CB, CB), cols_of(span)],
                recv_a.at[pl.ds(d * CB, CB), cols_of(span)],
                A, a_sem.at[q], plane[d],
            )

    def rs_start(src, rows, offs, dst_off, turn, minus, plus, span, send, sems, i):
        c0, c1 = span
        mid = (c0 + c1) // 2
        lo, hi = pl.ds(c0, mid - c0), pl.ds(mid, c1 - mid)
        cols = cols_of(span)
        o0, o1, o2, o3 = (pl.ds(o, rows) for o in offs)
        od = pl.ds(dst_off, rows)
        turn_lo, turn_hi, from_minus, from_plus = (sems.at[i + n] for n in range(4))
        start(src.at[o2, lo], turn.at[od, lo], send, turn_lo, right)
        start(src.at[o2, hi], turn.at[od, hi], send, turn_hi, left)
        start(src.at[o1, hi], minus.at[od, hi], send, from_minus, right)
        start(src.at[o3, lo], plus.at[od, lo], send, from_plus, left)

        def middle():
            arrived(turn.at[od, lo], turn_lo)
            src[o1, lo] = (src[o1, lo].astype(F32) + turn[od, lo].astype(F32)).astype(BF16)
            start(src.at[o1, lo], minus.at[od, lo], send, from_minus, right)
            arrived(turn.at[od, hi], turn_hi)
            src[o3, hi] = (src[o3, hi].astype(F32) + turn[od, hi].astype(F32)).astype(BF16)
            start(src.at[o3, hi], plus.at[od, hi], send, from_plus, left)

        def end():
            arrived(minus.at[od, cols], from_minus)
            arrived(plus.at[od, cols], from_plus)
            total = src[o0, cols].astype(F32) + minus[od, cols].astype(F32)
            return (total + plus[od, cols].astype(F32)).astype(BF16)

        return middle, end

    scoped("halo", arrived, halo, halo_sem.at[0])
    product[0:8, :] = jnp.where(ep == 0, 0.0, halo[...])
    convolved = jnp.zeros((tokens, p.C), F32)
    taps = conv_taps.shape[0]
    for k in range(taps):
        convolved = convolved + conv_taps[k : k + 1, :] * product[pl.ds(8 - taps + 1 + k, tokens), :]
    mixed[...] = (b_gate[...].astype(F32) * convolved).astype(BF16)
    scoped("wmix", loads[0].wait)
    m_rows = tokens // X
    for rel in range(X):
        own = pl.ds(pl.multiple_of(((x + rel) % X) * m_rows, m_rows), m_rows)
        m_part[pl.ds(rel * m_rows, m_rows), :] = jnp.dot(
            mixed[own, :], w_mix[...], preferred_element_type=F32
        ).astype(BF16)
    m_middle, m_end = rs_start(
        m_part, m_rows, [rel * m_rows for rel in range(X)], 0, m_turn, m_minus, m_plus, (0, D), MX, mx_sem, 0
    )

    scoped("m_mid", m_middle)

    def where(j, rel):
        return pl.ds(p.off(j // GS, rel, j % GS), CB)

    def turn_in(q):
        c0, c1 = p.QA[q]
        cols = cols_of(p.QA[q])
        with jax.named_scope(f"a_wait#{q}"):
            arrived(recv_a.at[pl.ds(CB, R - CB), cols], a_sem.at[q])
        step = min(256, D // 8)

        def tile(i, _):
            part_cols = pl.ds(pl.multiple_of(c0 + i * step, step), step)
            moved = jnp.dot(perm[...], recv_a[0:R, part_cols], preferred_element_type=F32)
            moved = moved.astype(BF16)
            send_b[0:R, part_cols] = moved
            gathered[0:CB, part_cols] = moved[0:CB]
            return 0

        scoped(f"turn_in#{q}", lambda: lax.fori_loop(0, (c1 - c0) // step, tile, 0))
        for j in p.by_distance[1:] if q == 0 else p.by_distance[:0:-1]:
            start(
                send_b.at[pl.ds(j * CB, CB), cols], gathered.at[where(j, 0), cols],
                B, b_sem.at[q * NZ + j], line[j],
            )

    def gather_out(q, j):
        cols = cols_of(p.QA[q])
        i = 2 * (q * NZ + j)
        own = gathered.at[where(j, 0), cols]
        if j:
            arrived(own, b_sem.at[q * NZ + j])
        start(own, gathered.at[where(j, 3), cols], AG, ag_sem.at[i], right)
        start(own, gathered.at[where(j, 1), cols], AG, ag_sem.at[i + 1], left)

    def gather_on(q, j):
        c0, c1 = p.QA[q]
        mid = (c0 + c1) // 2
        cols, lo, hi = cols_of(p.QA[q]), pl.ds(c0, mid - c0), pl.ds(mid, c1 - mid)
        i = 2 * (q * NZ + j)
        k = j // GS
        arrived(gathered.at[where(j, 3), cols], ag_sem.at[i])
        start(gathered.at[where(j, 3), lo], gathered.at[where(j, 2), lo], FW, fw_sem.at[k], right)
        arrived(gathered.at[where(j, 1), cols], ag_sem.at[i + 1])
        start(gathered.at[where(j, 1), hi], gathered.at[where(j, 2), hi], FW, fw_sem.at[k], left)

    rows_k = X * GS * CB

    def pieces(k):
        r0 = p.off(k, 0)

        def up(t, _):
            cols = pl.ds(pl.multiple_of(t * 128, 128), 128)
            pair = jnp.concatenate([w_gate[:, cols], w_up[:, cols]], axis=1)
            both = jnp.dot(gathered[r0 : r0 + rows_k, :], pair, preferred_element_type=F32)
            hid[:, cols] = (jax.nn.silu(both[:, :128]) * both[:, 128:]).astype(BF16)
            return 0

        def down(n, _):
            cols = pl.ds(pl.multiple_of(n * wide, wide), wide)
            out = jnp.dot(hid[...], w_down[:, cols], preferred_element_type=F32).astype(BF16)
            for rel in range(X):
                to = rel * R + k * GS * CB
                part[to : to + GS * CB, cols] = out[rel * GS * CB : (rel + 1) * GS * CB]
            return 0

        def first():
            with jax.named_scope(f"cwait#{k}"):
                arrived(gathered.at[pl.ds(p.off(k, 2), GS * CB), :], fw_sem.at[k])
                if k == NG - 1:
                    for copy in loads[1:]:
                        copy.wait()
            loop(up, 0, cuts[1])

        def loop(f, lo, hi):
            with jax.named_scope(f"{f.__name__}#{k},{lo}"):
                lax.fori_loop(lo, hi, f, 0)

        tiles, outs = F // 128, D // wide
        cuts = [0, (tiles + 2) // 3, (2 * tiles + 2) // 3, tiles]
        yield first
        yield lambda: loop(up, cuts[1], cuts[2])
        yield lambda: loop(up, cuts[2], cuts[3])
        yield lambda: loop(down, 0, (outs + 1) // 2)
        yield lambda: loop(down, (outs + 1) // 2, outs)

    rs = {}
    rows_h = R // 2

    def sum_start(n):
        h, q = units[n]
        rs[n] = rs_start(
            part, rows_h, [rel * R + h * rows_h for rel in range(X)], h * rows_h,
            turn, s_minus, s_plus, p.QR[q], RS, rs_sem, 4 * n,
        )

    def sum_end(n):
        h, q = units[n]
        total = rs[n][1]()
        cols = cols_of(p.QR[q])
        out_b[h * rows_h : (h + 1) * rows_h, cols] = total
        if h == 0:
            ret_b[0:CB, cols] = total[0:CB]
        first_j = h * NZ // 2
        for j in reversed(range(max(first_j, 1), first_j + NZ // 2)):
            rows = pl.ds(j * CB, CB)
            start(out_b.at[rows, cols], ret_b.at[rows, cols], RB, rb_sem.at[q], line_back[j])

    slot_j = lax.broadcasted_iota(jnp.int32, (T, R), 1)
    w_cols = [as_col(route_weights[k : k + 1, :]) for k in range(2)]
    mix = jnp.where(slot_j == slots[0], w_cols[0], 0.0)
    mix = mix + jnp.where(slot_j == slots[1], w_cols[1], 0.0)
    mix_hi[...] = mix.astype(BF16)
    mix_lo[...] = (mix - mix_hi[...].astype(F32)).astype(BF16)

    def turn_out(q):
        cols = cols_of(p.QR[q])
        with jax.named_scope(f"rb_wait#{q}"):
            arrived(ret_b.at[pl.ds(CB, R - CB), cols], rb_sem.at[q])
        with jax.named_scope(f"turn_out#{q}"):
            moved = jnp.dot(perm[...], ret_b[0:R, cols], preferred_element_type=F32).astype(BF16)
            send_r[0:R, cols] = moved
            ret_a[0:CB, cols] = moved[0:CB]
        for d in range(1, G):
            rows = pl.ds(d * CB, CB)
            start(send_r.at[rows, cols], ret_a.at[rows, cols], RA, ra_sem.at[q], plane_back[d])

    def combine(q):
        cols = cols_of(p.QR[q])
        with jax.named_scope(f"ra_wait#{q}"):
            arrived(ret_a.at[pl.ds(CB, R - CB), cols], ra_sem.at[q])
        with jax.named_scope(f"combine#{q}"):
            rows = ret_a[0:R, cols]
            total = jnp.dot(mix_hi[...], rows, preferred_element_type=F32)
            total = total + jnp.dot(mix_lo[...], rows, preferred_element_type=F32)
            moe_out[:, cols] = total.astype(BF16)

    near_first, lead = p.by_distance, NZ // 2
    steps = [(0, j) for j in near_first[:lead]] + [(0, near_first[lead]), (1, 0)]
    steps += [(0, j) for j in near_first[lead + 1 :]] + [(1, j) for j in range(NZ - 1, 0, -1)]
    work, computed, due = [], set(), []
    on = 0

    def do_work(count):
        while count and work:
            k, piece = work.pop(0)
            piece()
            count -= 1
            if k is not None:
                computed.add(k)

    def take(k):
        for n, piece in enumerate(pieces(k)):
            work.append((k if n == 4 else None, piece))

    def step_on():
        nonlocal on
        q, j = steps[on]
        scoped(f"gon#{q},{j}", gather_on, q, j)
        on += 1
        while due:
            take(due.pop(0))
        if q == 1 and j and (j % GS == 0 or j == 1):
            due.append(j // GS)

    turn_in(0)
    for n, (q, j) in enumerate(steps):
        if n == lead:
            turn_in(1)
        scoped(f"gout#{q},{j}", gather_out, q, j)
        ahead = 1 if n <= NZ else 2
        while on + ahead <= n:
            step_on()
            do_work(2)
    with jax.named_scope("m_end"):
        mixer_out[...] = m_end()
    while on < len(steps):
        step_on()
        do_work(2)
    while due:
        take(due.pop(0))
    last = len(p.QR) - 1
    far_units, near_units = [(1, q) for q in range(last + 1)], [(0, q) for q in range(last + 1)]
    units = far_units[:last] + near_units[:1] + far_units[last:] + near_units[1:]
    begun = 0
    for n in range(len(units) + 1):
        while begun < len(units) and begun <= n + 2:
            half_groups = range(NG // 2, NG) if units[begun][0] else range(NG // 2)
            if not computed.issuperset(half_groups):
                if begun > n and units[begun][0] == 0:
                    break
                while not computed.issuperset(half_groups):
                    do_work(1)
            scoped(f"sstart#{begun}", sum_start, begun)
            begun += 1
        if n < len(units):
            do_work(2)
            scoped(f"smid#{n}", rs[n][0])
        if n >= 1:
            scoped(f"send#{n - 1}", sum_end, n - 1)
            h, q = units[n - 1]
            if h == 0 and q:
                turn_out(q - 1)
                if q >= 2:
                    combine(q - 2)
    turn_out(last)
    combine(last - 1)
    combine(last)
    with jax.named_scope("sends"):
        sent(halo, HALO)
        sent(send_a.at[pl.ds(CB, R - CB), :], A)
        sent(send_b.at[pl.ds(CB, R - CB), :], B)
        sent(gathered.at[pl.ds(0, 2 * R), :], AG)
        sent(gathered.at[pl.ds(0, R), :], FW)
        sent(part.at[pl.ds(0, 3 * R), :], RS)
        sent(m_part.at[pl.ds(0, 3 * m_rows), :], MX)
        sent(out_b.at[pl.ds(CB, R - CB), :], RB)
        sent(send_r.at[pl.ds(CB, R - CB), :], RA)


def permutation(p):
    matrix = np.zeros((p.R, p.R), np.float32)
    for j in range(p.NZ):
        for d in range(p.G):
            for r in range(CAP):
                matrix[j * p.CB + d * CAP + r, d * p.CB + j * CAP + r] = 1.0
    return jnp.asarray(matrix, BF16)


def on_device(
    c_gate, b_gate, values, conv_taps, w_mix_out, moe_in, norm_gain,
    route_ids, route_weights, w_gate, w_up, w_down,
):
    n_ep, n_tp = lax.axis_size("ep"), lax.axis_size("tp")
    p = Plan(n_ep, n_tp, moe_in.shape[1], w_gate.shape[2], moe_in.shape[0], *c_gate.shape)
    D, F, T, R, CB, G, NZ, X = p.D, p.F, p.T, p.R, p.CB, p.G, p.NZ, p.X
    m_rows = p.TA // X
    vmem = pl.BlockSpec(memory_space=pltpu.VMEM)
    hbm = pl.BlockSpec(memory_space=pl.ANY)
    block = pltpu.VMEM((R + PAD, D), BF16)
    dma = pltpu.SemaphoreType.DMA
    return pl.pallas_call(
        functools.partial(body, p),
        name="mixer_and_experts",
        out_shape=(
            jax.ShapeDtypeStruct((m_rows, D), BF16),
            jax.ShapeDtypeStruct((T, D), BF16),
        ),
        in_specs=[vmem, vmem, vmem, vmem, hbm, vmem, vmem, vmem, vmem, vmem, hbm, hbm, hbm],
        out_specs=(vmem, vmem),
        scratch_shapes=[
            pltpu.VMEM(w_mix_out.shape, BF16),
            pltpu.VMEM((D, F), BF16),
            pltpu.VMEM((D, F), BF16),
            pltpu.VMEM((F, D), BF16),
            pltpu.VMEM((p.TA + 8, p.C), F32),
            pltpu.VMEM((8, p.C), F32),
            pltpu.VMEM((p.TA, p.C), BF16),
            pltpu.VMEM((p.TA, D), BF16),
            pltpu.VMEM((m_rows, D), BF16),
            pltpu.VMEM((m_rows, D), BF16),
            pltpu.VMEM((m_rows, D), BF16),
            pltpu.VMEM((T, D), BF16),
            block,
            block,
            block,
            pltpu.VMEM((X * R + PAD, D), BF16),
            pltpu.VMEM((X * p.GS * CB, F), BF16),
            pltpu.VMEM((X * R + PAD, D), BF16),
            block,
            block,
            block,
            block,
            block,
            block,
            block,
            pltpu.VMEM((T, R), BF16),
            pltpu.VMEM((T, R), BF16),
            dma((4,)),
            dma((9,)),
            dma((1,)),
            dma((len(p.QA),)),
            dma((len(p.QA) * NZ,)),
            dma((len(p.QA) * 2 * NZ,)),
            dma((p.NG,)),
            dma((4 * 2 * len(p.QR),)),
            dma((4,)),
            dma((len(p.QR),)),
            dma((len(p.QR),)),
        ],
        compiler_params=pltpu.CompilerParams(
            collective_id=0, has_side_effects=True, vmem_limit_bytes=60 * 2**20
        ),
    )(
        c_gate, b_gate, values, conv_taps, w_mix_out, moe_in, norm_gain.reshape(1, -1),
        route_ids.T, route_weights.T, permutation(p), w_gate, w_up, w_down,
    )


def solution(mesh):
    return jax.shard_map(
        on_device,
        mesh=mesh,
        in_specs=(
            P("ep", "tp"),
            P("ep", "tp"),
            P("ep", "tp"),
            P(None, "tp"),
            P("tp", None),
            P(("ep", "tp"), None),
            P(),
            P(("ep", "tp"), None),
            P(("ep", "tp"), None),
            P("ep", None, "tp"),
            P("ep", None, "tp"),
            P("ep", "tp", None),
        ),
        out_specs=(P(("ep", "tp"), None), P(("ep", "tp"), None)),
        check_vma=False,
    )
```

```python
import functools
import itertools

import jax
import jax.numpy as jnp
import numpy as np
from jax import lax
from jax.experimental import pallas as pl
from jax.experimental.pallas import tpu as pltpu
from jax.sharding import PartitionSpec as P

EPS = 1e-06
MESH = pl.DeviceIdType.MESH
F32 = jnp.float32
BF16 = jnp.bfloat16
CAP = 5
PAD = 8


class Plan:
    def __init__(self, n_ep, n_tp, width, hidden, rows, tokens, channels):
        self.G = int(round(n_ep**0.5))
        self.NZ = n_ep // self.G
        assert self.G * self.NZ == n_ep and self.G == self.NZ and n_tp == 4
        self.X = n_tp
        self.D, self.F, self.T = width, hidden, rows
        self.TA, self.C = tokens, channels
        self.CB = CAP * self.G
        self.R = self.CB * self.NZ
        self.GS = 2
        self.NG = self.NZ // self.GS
        far = self.NZ // 2
        self.dz = [0]
        for step in range(1, far - 1):
            self.dz += [-step, step]
        self.dz += [far, 1 - far, far - 1]
        assert len(self.dz) == self.NZ
        near_first = sorted(range(1, self.NZ), key=lambda j: abs(self.dz[j]))
        self.sends = [near_first, [1, 2] + list(range(self.NZ - 1, 2, -1))]
        eighth = width // 8
        self.QA = spans([2 * eighth, 6 * eighth])
        self.QR = spans([3 * eighth, 2 * eighth, 2 * eighth, eighth])
        self.QF = spans([5 * eighth, 3 * eighth])
        assert self.NZ == 8

    def off(self, k, rel, jj=0):
        return ((k * self.X + rel) * self.GS + jj) * self.CB


def spans(widths):
    ends = list(itertools.accumulate(widths))
    return [(end - width, end) for width, end in zip(widths, ends)]


def scoped(name, f, *a):
    with jax.named_scope(name):
        return f(*a)


def body(
    p,
    c_gate,
    b_gate,
    values,
    conv_taps,
    w_mix_hbm,
    moe_in,
    norm_gain,
    route_ids,
    route_weights,
    perm,
    w_gate_hbm,
    w_up_hbm,
    w_down_hbm,
    mixer_out,
    moe_out,
    w_mix,
    w_gate,
    w_up,
    w_down,
    product,
    halo,
    mixed,
    m_part,
    m_turn,
    m_minus,
    m_plus,
    normed,
    send_a,
    recv_a,
    send_b,
    gathered,
    hid,
    part,
    turn,
    s_minus,
    s_plus,
    out_b,
    ret_b,
    send_r,
    ret_a,
    mix_hi,
    mix_lo,
    w_sem,
    send_sem,
    halo_sem,
    a_sem,
    b_sem,
    ag_sem,
    fw_sem,
    rs_sem,
    mx_sem,
    rb_sem,
    ra_sem,
):
    G, NZ, X, D, F, T, CB, R, GS, NG = p.G, p.NZ, p.X, p.D, p.F, p.T, p.CB, p.R, p.GS, p.NG
    ep, x = lax.axis_index("ep"), lax.axis_index("tp")
    z, g = ep // G, ep % G

    def at(zz, gg, xx):
        return {"ep": zz * G + gg, "tp": xx}

    right, left = at(z, g, (x + 1) % X), at(z, g, (x + X - 1) % X)
    after = {"ep": (ep + 1) % (G * NZ), "tp": x}
    before = {"ep": (ep + G * NZ - 1) % (G * NZ), "tp": x}
    plane = [at(z, (g + d) % G, x) for d in range(G)]
    plane_back = [at(z, (g + G - d) % G, x) for d in range(G)]
    line = [at((z + NZ + dz) % NZ, g, x) for dz in p.dz]
    line_back = [at((z + NZ - dz) % NZ, g, x) for dz in p.dz]

    barrier = pltpu.get_barrier_semaphore()
    peers = plane[1:] + line[1:] + [right, left, after, before]
    for peer in peers:
        pl.semaphore_signal(barrier, inc=1, device_id=peer, device_id_type=MESH)

    def load(src, dst, i):
        copy = pltpu.make_async_copy(src, dst, w_sem.at[i])
        copy.start()
        return copy

    loads = [
        load(w_mix_hbm, w_mix, 0),
        load(w_gate_hbm.at[0], w_gate, 1),
        load(w_up_hbm.at[0], w_up, 2),
        load(w_down_hbm.at[0], w_down, 3),
    ]
    def start(src, dst, send, recv, peer):
        copy = pltpu.make_async_remote_copy(
            src_ref=src,
            dst_ref=dst,
            send_sem=send_sem.at[send],
            recv_sem=recv,
            device_id=peer,
            device_id_type=MESH,
        )
        copy.start()
        return copy

    def arrived(ref, recv):
        pltpu.make_async_remote_copy(
            src_ref=ref, dst_ref=ref, send_sem=send_sem.at[0], recv_sem=recv,
            device_id=right, device_id_type=MESH,
        ).wait_recv()

    def sent(ref, send):
        pltpu.make_async_remote_copy(
            src_ref=ref, dst_ref=ref, send_sem=send_sem.at[send], recv_sem=halo_sem.at[0],
            device_id=right, device_id_type=MESH,
        ).wait_send()

    HALO, A, B, AG, FW, RS, MX, RB, RA = range(9)

    tokens = p.TA
    product[8 : 8 + tokens, :] = c_gate[...].astype(F32) * values[...].astype(F32)

    stream = moe_in[...].astype(F32)
    scale = lax.rsqrt(jnp.mean(stream * stream, axis=1, keepdims=True) + EPS)
    normed[...] = (stream * scale * norm_gain[...]).astype(BF16)

    rows_i = lax.broadcasted_iota(jnp.int32, (T, T), 0)
    cols_i = lax.broadcasted_iota(jnp.int32, (T, T), 1)
    eye, earlier = rows_i == cols_i, cols_i < rows_i

    def as_row(col):
        return jnp.sum(jnp.where(eye, col, 0.0), axis=0, keepdims=True)

    def as_col(row):
        return jnp.sum(jnp.where(eye, row, 0.0), axis=1, keepdims=True)

    id_rows = [route_ids[k : k + 1, :].astype(F32) for k in range(2)]
    slots = []
    for col in [as_col(row) for row in id_rows]:
        seen = jnp.zeros((T, 1), F32)
        for row in id_rows:
            seen = seen + jnp.sum(
                jnp.where(earlier & (col == row), 1.0, 0.0), axis=1, keepdims=True
            )
        rank, expert = seen.astype(jnp.int32), col.astype(jnp.int32)
        to_g = (expert & (G - 1)) - g
        to_g = jnp.where(to_g < 0, to_g + G, to_g)
        to_z = (expert >> (G.bit_length() - 1)) - z
        to_z = jnp.where(to_z < 0, to_z + NZ, to_z)
        slot_z = jnp.zeros_like(to_z)
        for j, dz in enumerate(p.dz):
            slot_z = jnp.where(to_z == dz % NZ, j, slot_z)
        slots.append(to_g * CB + slot_z * CAP + rank)
    slot_rows = [as_row(col.astype(F32)).astype(jnp.int32) for col in slots]
    slot_i = lax.broadcasted_iota(jnp.int32, (R, T), 0)
    pick = jnp.where((slot_i == slot_rows[0]) | (slot_i == slot_rows[1]), 1.0, 0.0).astype(BF16)
    wide = min(512, D)

    def pack(i, _):
        cols = pl.ds(pl.multiple_of(i * wide, wide), wide)
        packed = jnp.dot(pick, normed[:, cols], preferred_element_type=F32).astype(BF16)
        send_a[0:R, cols] = packed
        recv_a[0:CB, cols] = packed[0:CB]
        return 0

    scoped("pack", lambda: lax.fori_loop(0, D // wide, pack, 0))

    def convolve(first, count):
        taps = conv_taps.shape[0]
        convolved = jnp.zeros((count, p.C), F32)
        for k in range(taps):
            reach = product[8 - taps + 1 + k + first : 8 - taps + 1 + k + first + count, :]
            convolved = convolved + conv_taps[k : k + 1, :] * reach
        return (b_gate[first : first + count, :].astype(F32) * convolved).astype(BF16)

    product[0:8, :] = jnp.zeros((8, p.C), F32)
    mixed[...] = convolve(0, tokens)
    scoped("wmix", loads[0].wait)
    m_rows = tokens // X
    for rel in range(X):
        own = pl.ds(pl.multiple_of(((x + rel) % X) * m_rows, m_rows), m_rows)
        m_part[pl.ds(rel * m_rows, m_rows), :] = jnp.dot(
            mixed[own, :], w_mix[...], preferred_element_type=F32
        ).astype(BF16)
    scoped("barrier", pl.semaphore_wait, barrier, len(peers))

    start(product.at[pl.ds(tokens, 8)], halo, HALO, halo_sem.at[0], after)

    def cols_of(span):
        return pl.ds(span[0], span[1] - span[0])

    def send_out(q):
        cols = cols_of(p.QA[q])
        for d in range(1, G):
            rows = pl.ds(d * CB, CB)
            start(send_a.at[rows, cols], recv_a.at[rows, cols], A + 9 * q, a_sem.at[q], plane[d])

    send_out(0)

    def rs_start(src, rows, offs, dst_off, turn, minus, plus, span, send, sems, i):
        c0, c1 = span
        mid = (c0 + c1) // 2
        lo, hi = pl.ds(c0, mid - c0), pl.ds(mid, c1 - mid)
        cols = cols_of(span)
        o0, o1, o2, o3 = (pl.ds(o, rows) for o in offs)
        od = pl.ds(dst_off, rows)
        turn_lo, turn_hi, from_minus, from_plus = (sems.at[i + n] for n in range(4))
        start(src.at[o2, lo], turn.at[od, lo], send, turn_lo, right)
        start(src.at[o2, hi], turn.at[od, hi], send, turn_hi, left)
        start(src.at[o1, hi], minus.at[od, hi], send, from_minus, right)
        start(src.at[o3, lo], plus.at[od, lo], send, from_plus, left)

        def middle():
            arrived(turn.at[od, lo], turn_lo)
            src[o1, lo] = (src[o1, lo].astype(F32) + turn[od, lo].astype(F32)).astype(BF16)
            start(src.at[o1, lo], minus.at[od, lo], send, from_minus, right)
            arrived(turn.at[od, hi], turn_hi)
            src[o3, hi] = (src[o3, hi].astype(F32) + turn[od, hi].astype(F32)).astype(BF16)
            start(src.at[o3, hi], plus.at[od, hi], send, from_plus, left)

        def end():
            arrived(minus.at[od, cols], from_minus)
            arrived(plus.at[od, cols], from_plus)
            total = src[o0, cols].astype(F32) + minus[od, cols].astype(F32)
            return (total + plus[od, cols].astype(F32)).astype(BF16)

        return middle, end

    scoped("halo", arrived, halo, halo_sem.at[0])
    product[0:8, :] = jnp.where(ep == 0, 0.0, halo[...])
    top = 16
    mixed[0:top, :] = convolve(0, top)
    to_top = pl.multiple_of(((X - x) % X) * m_rows, m_rows)
    m_part[pl.ds(to_top, top), :] = jnp.dot(
        mixed[0:top, :], w_mix[...], preferred_element_type=F32
    ).astype(BF16)
    m_middle, m_end = rs_start(
        m_part, m_rows, [rel * m_rows for rel in range(X)], 0, m_turn, m_minus, m_plus, (0, D), MX, mx_sem, 0
    )

    with jax.named_scope("a_sent"):
        sent(send_a.at[pl.ds(CB, R - CB), cols_of(p.QA[0])], A)
    send_out(1)
    scoped("m_mid", m_middle)

    def where(j, rel):
        return pl.ds(p.off(j // GS, rel, j % GS), CB)

    def turn_in(q):
        c0, c1 = p.QA[q]
        cols = cols_of(p.QA[q])
        with jax.named_scope(f"a_wait#{q}"):
            arrived(recv_a.at[pl.ds(CB, R - CB), cols], a_sem.at[q])
        step = min(256, D // 8)

        def tile(i, _):
            part_cols = pl.ds(pl.multiple_of(c0 + i * step, step), step)
            moved = jnp.dot(perm[...], recv_a[0:R, part_cols], preferred_element_type=F32)
            moved = moved.astype(BF16)
            send_b[0:R, part_cols] = moved
            gathered[0:CB, part_cols] = moved[0:CB]
            return 0

        scoped(f"turn_in#{q}", lambda: lax.fori_loop(0, (c1 - c0) // step, tile, 0))
        for j in p.sends[q]:
            start(
                send_b.at[pl.ds(j * CB, CB), cols], gathered.at[where(j, 0), cols],
                B, b_sem.at[q * NZ + j], line[j],
            )

    def gather_out(q, j):
        cols = cols_of(p.QA[q])
        i = 2 * (q * NZ + j)
        own = gathered.at[where(j, 0), cols]
        if j:
            arrived(own, b_sem.at[q * NZ + j])
        start(own, gathered.at[where(j, 3), cols], AG, ag_sem.at[i], right)
        start(own, gathered.at[where(j, 1), cols], AG, ag_sem.at[i + 1], left)

    def gather_on(q, j):
        c0, c1 = p.QA[q]
        mid = (c0 + c1) // 2
        cols, lo, hi = cols_of(p.QA[q]), pl.ds(c0, mid - c0), pl.ds(mid, c1 - mid)
        i = 2 * (q * NZ + j)
        k = j // GS
        arrived(gathered.at[where(j, 3), cols], ag_sem.at[i])
        start(gathered.at[where(j, 3), lo], gathered.at[where(j, 2), lo], FW, fw_sem.at[k], right)
        arrived(gathered.at[where(j, 1), cols], ag_sem.at[i + 1])
        start(gathered.at[where(j, 1), hi], gathered.at[where(j, 2), hi], FW, fw_sem.at[k], left)

    rows_k = X * GS * CB

    def pieces(k):
        r0 = p.off(k, 0)

        def up(t, _):
            cols = pl.ds(pl.multiple_of(t * 128, 128), 128)
            pair = jnp.concatenate([w_gate[:, cols], w_up[:, cols]], axis=1)
            both = jnp.dot(gathered[r0 : r0 + rows_k, :], pair, preferred_element_type=F32)
            hid[:, cols] = (jax.nn.silu(both[:, :128]) * both[:, 128:]).astype(BF16)
            return 0

        def down(n, _):
            cols = pl.ds(pl.multiple_of(n * (D // 2), 128), D // 2)
            out = jnp.dot(hid[...], w_down[:, cols], preferred_element_type=F32).astype(BF16)
            for rel in range(X):
                to = rel * R + k * GS * CB
                part[to : to + GS * CB, cols] = out[rel * GS * CB : (rel + 1) * GS * CB]
            return 0

        def first():
            with jax.named_scope(f"cwait#{k}"):
                arrived(gathered.at[pl.ds(p.off(k, 2), GS * CB), :], fw_sem.at[k])
                if k == 0:
                    for copy in loads[1:]:
                        copy.wait()
            loop(up, 0, cuts[1])

        def loop(f, lo, hi):
            with jax.named_scope(f"{f.__name__}#{k},{lo}"):
                lax.fori_loop(lo, hi, f, 0)

        tiles, outs = F // 128, 2
        cuts = [0, (tiles + 2) // 3, (2 * tiles + 2) // 3, tiles]
        yield first
        yield lambda: loop(up, cuts[1], cuts[2])
        yield lambda: loop(up, cuts[2], cuts[3])
        yield lambda: loop(down, 0, (outs + 1) // 2)
        yield lambda: loop(down, (outs + 1) // 2, outs)

    rs = {}
    half = NZ // 2
    far_units = [(k * GS, GS, span) for span in p.QF for k in range(NG - 1, NG // 2 - 1, -1)]
    units = far_units + [(0, half, span) for span in p.QR]
    units = units[:2] + units[4:5] + units[2:4] + units[5:]

    def sum_start(n):
        j, count, span = units[n]
        rs[n] = rs_start(
            part, count * CB, [rel * R + j * CB for rel in range(X)], j * CB,
            turn, s_minus, s_plus, span, RS, rs_sem, 4 * n,
        )

    def back_sem(n):
        span = units[n][2]
        return rb_sem.at[p.QF.index(span)] if units[n][0] else rb_sem.at[len(p.QF) + p.QR.index(span)]

    def sum_end(n):
        j0, count, span = units[n]
        total = rs[n][1]()
        cols = cols_of(span)
        out_b[j0 * CB : (j0 + count) * CB, cols] = total
        if j0 == 0:
            ret_b[0:CB, cols] = total[0:CB]
        for j in reversed(range(max(j0, 1), j0 + count)):
            rows = pl.ds(j * CB, CB)
            start(out_b.at[rows, cols], ret_b.at[rows, cols], RB, back_sem(n), line_back[j])

    far_back = set()
    slot_j = lax.broadcasted_iota(jnp.int32, (T, R), 1)
    w_cols = [as_col(route_weights[k : k + 1, :]) for k in range(2)]
    mix = jnp.where(slot_j == slots[0], w_cols[0], 0.0)
    mix = mix + jnp.where(slot_j == slots[1], w_cols[1], 0.0)
    mix_hi[...] = mix.astype(BF16)
    mix_lo[...] = (mix - mix_hi[...].astype(F32)).astype(BF16)

    def turn_out(q):
        cols = cols_of(p.QR[q])
        with jax.named_scope(f"rb_wait#{q}"):
            for i, span in enumerate(p.QF):
                if span[0] < p.QR[q][1] and i not in far_back:
                    far_back.add(i)
                    arrived(ret_b.at[pl.ds(half * CB, R - half * CB), cols_of(span)], rb_sem.at[i])
            arrived(ret_b.at[pl.ds(CB, (half - 1) * CB), cols], rb_sem.at[len(p.QF) + q])
        with jax.named_scope(f"turn_out#{q}"):
            moved = jnp.dot(perm[...], ret_b[0:R, cols], preferred_element_type=F32).astype(BF16)
            send_r[0:R, cols] = moved
            ret_a[0:CB, cols] = moved[0:CB]
        for d in range(1, G):
            rows = pl.ds(d * CB, CB)
            start(send_r.at[rows, cols], ret_a.at[rows, cols], RA, ra_sem.at[q], plane_back[d])

    def combine(q):
        cols = cols_of(p.QR[q])
        with jax.named_scope(f"ra_wait#{q}"):
            arrived(ret_a.at[pl.ds(CB, R - CB), cols], ra_sem.at[q])
        with jax.named_scope(f"combine#{q}"):
            rows = ret_a[0:R, cols]
            total = jnp.dot(mix_hi[...], rows, preferred_element_type=F32)
            total = total + jnp.dot(mix_lo[...], rows, preferred_element_type=F32)
            moe_out[:, cols] = total.astype(BF16)

    work, computed = [], set()

    def do_work(count):
        while count and work:
            k, n, piece = work.pop(0)
            piece()
            count -= 1
            if n == 4:
                computed.add(k)

    script = """
        t0 o00 o01 n00 o02 n01 o03 n02 o04 t1 n03 o10 o06 o07 n04 n06 n07 o05 n10 n05
        o11 o12 n11 o17 o16 n12 w0 c1 n17 o15 c1 n16 c2 o14 o13 c1 n15 w3 c1 n14 c2 n13 c2
        s0 m w2 c3 i0 c2 s1 w1 c3 i1 c2 s2
    """
    for event in script.split():
        kind, at_n = event[0], [int(digit) for digit in event[1:]]
        if kind == "t":
            turn_in(*at_n)
        elif kind == "o":
            scoped("gout#" + event, gather_out, *at_n)
        elif kind == "n":
            scoped("gon#" + event, gather_on, *at_n)
        elif kind == "w":
            work.extend((at_n[0], n, piece) for n, piece in enumerate(pieces(at_n[0])))
        elif kind == "c":
            do_work(*at_n)
        elif kind == "s":
            scoped("sstart#" + event, sum_start, *at_n)
        elif kind == "i":
            scoped("smid#" + event, rs[at_n[0]][0])
        elif kind == "m":
            with jax.named_scope("m_end"):
                mixer_out[...] = m_end()
    last, turns = len(p.QR) - 1, {4: 0}
    begun = 3
    for n in range(len(units) + 1):
        while begun < len(units) and begun <= n + 2:
            scoped(f"sstart#{begun}", sum_start, begun)
            begun += 1
        if 2 <= n < len(units):
            scoped(f"smid#{n}", rs[n][0])
        if n >= 1:
            scoped(f"send#{n - 1}", sum_end, n - 1)
        if n - 1 in turns:
            turn_out(turns[n - 1])
    turn_out(1)
    turn_out(2)
    turn_out(last)
    for q in range(last + 1):
        combine(q)
    with jax.named_scope("sends"):
        sent(halo, HALO)
        sent(send_a.at[pl.ds(CB, R - CB), cols_of(p.QA[1])], A + 9)
        sent(send_b.at[pl.ds(CB, R - CB), :], B)
        sent(gathered.at[pl.ds(0, 2 * R), :], AG)
        sent(gathered.at[pl.ds(0, R), :], FW)
        sent(part.at[pl.ds(0, 3 * R), :], RS)
        sent(m_part.at[pl.ds(0, 3 * m_rows), :], MX)
        sent(out_b.at[pl.ds(CB, R - CB), :], RB)
        sent(send_r.at[pl.ds(CB, R - CB), :], RA)


def permutation(p):
    matrix = np.zeros((p.R, p.R), np.float32)
    for j in range(p.NZ):
        for d in range(p.G):
            for r in range(CAP):
                matrix[j * p.CB + d * CAP + r, d * p.CB + j * CAP + r] = 1.0
    return jnp.asarray(matrix, BF16)


def on_device(
    c_gate, b_gate, values, conv_taps, w_mix_out, moe_in, norm_gain,
    route_ids, route_weights, w_gate, w_up, w_down,
):
    n_ep, n_tp = lax.axis_size("ep"), lax.axis_size("tp")
    p = Plan(n_ep, n_tp, moe_in.shape[1], w_gate.shape[2], moe_in.shape[0], *c_gate.shape)
    D, F, T, R, CB, G, NZ, X = p.D, p.F, p.T, p.R, p.CB, p.G, p.NZ, p.X
    m_rows = p.TA // X
    vmem = pl.BlockSpec(memory_space=pltpu.VMEM)
    hbm = pl.BlockSpec(memory_space=pl.ANY)
    block = pltpu.VMEM((R + PAD, D), BF16)
    dma = pltpu.SemaphoreType.DMA
    return pl.pallas_call(
        functools.partial(body, p),
        name="mixer_and_experts",
        out_shape=(
            jax.ShapeDtypeStruct((m_rows, D), BF16),
            jax.ShapeDtypeStruct((T, D), BF16),
        ),
        in_specs=[vmem, vmem, vmem, vmem, hbm, vmem, vmem, vmem, vmem, vmem, hbm, hbm, hbm],
        out_specs=(vmem, vmem),
        scratch_shapes=[
            pltpu.VMEM(w_mix_out.shape, BF16),
            pltpu.VMEM((D, F), BF16),
            pltpu.VMEM((D, F), BF16),
            pltpu.VMEM((F, D), BF16),
            pltpu.VMEM((p.TA + 8, p.C), F32),
            pltpu.VMEM((8, p.C), F32),
            pltpu.VMEM((p.TA, p.C), BF16),
            pltpu.VMEM((p.TA, D), BF16),
            pltpu.VMEM((m_rows, D), BF16),
            pltpu.VMEM((m_rows, D), BF16),
            pltpu.VMEM((m_rows, D), BF16),
            pltpu.VMEM((T, D), BF16),
            block,
            block,
            block,
            pltpu.VMEM((X * R + PAD, D), BF16),
            pltpu.VMEM((X * p.GS * CB, F), BF16),
            pltpu.VMEM((X * R + PAD, D), BF16),
            block,
            block,
            block,
            block,
            block,
            block,
            block,
            pltpu.VMEM((T, R), BF16),
            pltpu.VMEM((T, R), BF16),
            dma((4,)),
            dma((11,)),
            dma((1,)),
            dma((len(p.QA),)),
            dma((len(p.QA) * NZ,)),
            dma((len(p.QA) * 2 * NZ,)),
            dma((p.NG,)),
            dma((4 * (p.NG // 2 * len(p.QF) + len(p.QR)),)),
            dma((4,)),
            dma((len(p.QF) + len(p.QR),)),
            dma((len(p.QR),)),
        ],
        compiler_params=pltpu.CompilerParams(
            collective_id=0, has_side_effects=True, vmem_limit_bytes=60 * 2**20
        ),
    )(
        c_gate, b_gate, values, conv_taps, w_mix_out, moe_in, norm_gain.reshape(1, -1),
        route_ids.T, route_weights.T, permutation(p), w_gate, w_up, w_down,
    )


def solution(mesh):
    return jax.shard_map(
        on_device,
        mesh=mesh,
        in_specs=(
            P("ep", "tp"),
            P("ep", "tp"),
            P("ep", "tp"),
            P(None, "tp"),
            P("tp", None),
            P(("ep", "tp"), None),
            P(),
            P(("ep", "tp"), None),
            P(("ep", "tp"), None),
            P("ep", None, "tp"),
            P("ep", None, "tp"),
            P("ep", "tp", None),
        ),
        out_specs=(P(("ep", "tp"), None), P(("ep", "tp"), None)),
        check_vma=False,
    )
```

```python
import functools
import itertools

import jax
import jax.numpy as jnp
import numpy as np
from jax import lax
from jax.experimental import pallas as pl
from jax.experimental.pallas import tpu as pltpu
from jax.sharding import PartitionSpec as P

EPS = 1e-06
MESH = pl.DeviceIdType.MESH
F32 = jnp.float32
BF16 = jnp.bfloat16
CAP = 5
PAD = 8


class Plan:
    def __init__(self, n_ep, n_tp, width, hidden, rows, tokens, channels):
        self.G = int(round(n_ep**0.5))
        self.NZ = n_ep // self.G
        assert self.G * self.NZ == n_ep and self.G == self.NZ and n_tp == 4
        self.X = n_tp
        self.D, self.F, self.T = width, hidden, rows
        self.TA, self.C = tokens, channels
        self.CB = CAP * self.G
        self.R = self.CB * self.NZ
        self.GS = 2
        self.NG = self.NZ // self.GS
        far = self.NZ // 2
        self.dz = [0]
        for step in range(1, far - 1):
            self.dz += [-step, step]
        self.dz += [far, 1 - far, far - 1]
        assert len(self.dz) == self.NZ
        near_first = sorted(range(1, self.NZ), key=lambda j: abs(self.dz[j]))
        self.sends = [near_first, [1, 2] + list(range(self.NZ - 1, 2, -1))]
        eighth = width // 8
        self.QA = spans([3 * eighth, 5 * eighth])
        self.QR = spans([4 * eighth, 2 * eighth, eighth, eighth])
        self.QF = spans([6 * eighth, 2 * eighth])
        assert self.NZ == 8

    def off(self, k, rel, jj=0):
        return ((k * self.X + rel) * self.GS + jj) * self.CB


def spans(widths):
    ends = list(itertools.accumulate(widths))
    return [(end - width, end) for width, end in zip(widths, ends)]


def scoped(name, f, *a):
    with jax.named_scope(name):
        return f(*a)


def body(
    p,
    c_gate,
    b_gate,
    values,
    conv_taps,
    w_mix_hbm,
    moe_in,
    norm_gain,
    route_ids,
    route_weights,
    perm,
    w_gate_hbm,
    w_up_hbm,
    w_down_hbm,
    mixer_out,
    moe_out,
    w_mix,
    w_gate,
    w_up,
    w_down,
    product,
    halo,
    mixed,
    m_part,
    m_turn,
    m_minus,
    m_plus,
    normed,
    send_a,
    recv_a,
    send_b,
    gathered,
    hid,
    part,
    turn,
    s_minus,
    s_plus,
    out_b,
    ret_b,
    send_r,
    ret_a,
    mix_hi,
    mix_lo,
    w_sem,
    send_sem,
    halo_sem,
    a_sem,
    b_sem,
    ag_sem,
    fw_sem,
    rs_sem,
    mx_sem,
    rb_sem,
    ra_sem,
):
    G, NZ, X, D, F, T, CB, R, GS, NG = p.G, p.NZ, p.X, p.D, p.F, p.T, p.CB, p.R, p.GS, p.NG
    ep, x = lax.axis_index("ep"), lax.axis_index("tp")
    z, g = ep // G, ep % G

    def at(zz, gg, xx):
        return {"ep": zz * G + gg, "tp": xx}

    right, left = at(z, g, (x + 1) % X), at(z, g, (x + X - 1) % X)
    after = {"ep": (ep + 1) % (G * NZ), "tp": x}
    before = {"ep": (ep + G * NZ - 1) % (G * NZ), "tp": x}
    plane = [at(z, (g + d) % G, x) for d in range(G)]
    plane_back = [at(z, (g + G - d) % G, x) for d in range(G)]
    line = [at((z + NZ + dz) % NZ, g, x) for dz in p.dz]
    line_back = [at((z + NZ - dz) % NZ, g, x) for dz in p.dz]

    barrier = pltpu.get_barrier_semaphore()
    peers = plane[1:] + line[1:] + [right, left, after, before]
    for peer in peers:
        pl.semaphore_signal(barrier, inc=1, device_id=peer, device_id_type=MESH)

    def load(src, dst, i):
        copy = pltpu.make_async_copy(src, dst, w_sem.at[i])
        copy.start()
        return copy

    loads = [
        load(w_mix_hbm, w_mix, 0),
        load(w_gate_hbm.at[0], w_gate, 1),
        load(w_up_hbm.at[0], w_up, 2),
        load(w_down_hbm.at[0], w_down, 3),
    ]
    def start(src, dst, send, recv, peer):
        copy = pltpu.make_async_remote_copy(
            src_ref=src,
            dst_ref=dst,
            send_sem=send_sem.at[send],
            recv_sem=recv,
            device_id=peer,
            device_id_type=MESH,
        )
        copy.start()
        return copy

    def arrived(ref, recv):
        pltpu.make_async_remote_copy(
            src_ref=ref, dst_ref=ref, send_sem=send_sem.at[0], recv_sem=recv,
            device_id=right, device_id_type=MESH,
        ).wait_recv()

    def sent(ref, send):
        pltpu.make_async_remote_copy(
            src_ref=ref, dst_ref=ref, send_sem=send_sem.at[send], recv_sem=halo_sem.at[0],
            device_id=right, device_id_type=MESH,
        ).wait_send()

    HALO, A, B, AG, FW, RS, MX, RB, RA = range(9)

    tokens = p.TA
    product[8 : 8 + tokens, :] = c_gate[...].astype(F32) * values[...].astype(F32)

    stream = moe_in[...].astype(F32)
    scale = lax.rsqrt(jnp.mean(stream * stream, axis=1, keepdims=True) + EPS)
    normed[...] = (stream * scale * norm_gain[...]).astype(BF16)

    rows_i = lax.broadcasted_iota(jnp.int32, (T, T), 0)
    cols_i = lax.broadcasted_iota(jnp.int32, (T, T), 1)
    eye, earlier = rows_i == cols_i, cols_i < rows_i

    def as_row(col):
        return jnp.sum(jnp.where(eye, col, 0.0), axis=0, keepdims=True)

    def as_col(row):
        return jnp.sum(jnp.where(eye, row, 0.0), axis=1, keepdims=True)

    id_rows = [route_ids[k : k + 1, :].astype(F32) for k in range(2)]
    slots = []
    for col in [as_col(row) for row in id_rows]:
        seen = jnp.zeros((T, 1), F32)
        for row in id_rows:
            seen = seen + jnp.sum(
                jnp.where(earlier & (col == row), 1.0, 0.0), axis=1, keepdims=True
            )
        rank, expert = seen.astype(jnp.int32), col.astype(jnp.int32)
        to_g = (expert & (G - 1)) - g
        to_g = jnp.where(to_g < 0, to_g + G, to_g)
        to_z = (expert >> (G.bit_length() - 1)) - z
        to_z = jnp.where(to_z < 0, to_z + NZ, to_z)
        slot_z = jnp.zeros_like(to_z)
        for j, dz in enumerate(p.dz):
            slot_z = jnp.where(to_z == dz % NZ, j, slot_z)
        slots.append(to_g * CB + slot_z * CAP + rank)
    slot_rows = [as_row(col.astype(F32)).astype(jnp.int32) for col in slots]
    slot_i = lax.broadcasted_iota(jnp.int32, (R, T), 0)
    pick = jnp.where((slot_i == slot_rows[0]) | (slot_i == slot_rows[1]), 1.0, 0.0).astype(BF16)
    wide = min(512, D)

    def pack(i, _):
        cols = pl.ds(pl.multiple_of(i * wide, wide), wide)
        packed = jnp.dot(pick, normed[:, cols], preferred_element_type=F32).astype(BF16)
        send_a[0:R, cols] = packed
        recv_a[0:CB, cols] = packed[0:CB]
        return 0

    scoped("pack", lambda: lax.fori_loop(0, D // wide, pack, 0))

    def convolve(first, count):
        taps = conv_taps.shape[0]
        convolved = jnp.zeros((count, p.C), F32)
        for k in range(taps):
            reach = product[8 - taps + 1 + k + first : 8 - taps + 1 + k + first + count, :]
            convolved = convolved + conv_taps[k : k + 1, :] * reach
        return (b_gate[first : first + count, :].astype(F32) * convolved).astype(BF16)

    product[0:8, :] = jnp.zeros((8, p.C), F32)
    mixed[...] = convolve(0, tokens)
    scoped("wmix", loads[0].wait)
    m_rows = tokens // X
    for rel in range(X):
        own = pl.ds(pl.multiple_of(((x + rel) % X) * m_rows, m_rows), m_rows)
        m_part[pl.ds(rel * m_rows, m_rows), :] = jnp.dot(
            mixed[own, :], w_mix[...], preferred_element_type=F32
        ).astype(BF16)
    scoped("barrier", pl.semaphore_wait, barrier, len(peers))

    start(product.at[pl.ds(tokens, 8)], halo, HALO, halo_sem.at[0], after)

    def cols_of(span):
        return pl.ds(span[0], span[1] - span[0])

    def send_out(q):
        cols = cols_of(p.QA[q])
        for d in range(1, G):
            rows = pl.ds(d * CB, CB)
            start(send_a.at[rows, cols], recv_a.at[rows, cols], A + 9 * q, a_sem.at[q], plane[d])

    send_out(0)

    def rs_start(src, rows, offs, dst_off, turn, minus, plus, span, send, sems, i):
        c0, c1 = span
        mid = (c0 + c1) // 2
        lo, hi = pl.ds(c0, mid - c0), pl.ds(mid, c1 - mid)
        cols = cols_of(span)
        o0, o1, o2, o3 = (pl.ds(o, rows) for o in offs)
        od = pl.ds(dst_off, rows)
        turn_lo, turn_hi, from_minus, from_plus = (sems.at[i + n] for n in range(4))
        start(src.at[o2, lo], turn.at[od, lo], send, turn_lo, right)
        start(src.at[o2, hi], turn.at[od, hi], send, turn_hi, left)
        start(src.at[o1, hi], minus.at[od, hi], send, from_minus, right)
        start(src.at[o3, lo], plus.at[od, lo], send, from_plus, left)

        def middle():
            arrived(turn.at[od, lo], turn_lo)
            src[o1, lo] = (src[o1, lo].astype(F32) + turn[od, lo].astype(F32)).astype(BF16)
            start(src.at[o1, lo], minus.at[od, lo], send, from_minus, right)
            arrived(turn.at[od, hi], turn_hi)
            src[o3, hi] = (src[o3, hi].astype(F32) + turn[od, hi].astype(F32)).astype(BF16)
            start(src.at[o3, hi], plus.at[od, hi], send, from_plus, left)

        def end():
            arrived(minus.at[od, cols], from_minus)
            arrived(plus.at[od, cols], from_plus)
            total = src[o0, cols].astype(F32) + minus[od, cols].astype(F32)
            return (total + plus[od, cols].astype(F32)).astype(BF16)

        return middle, end

    scoped("halo", arrived, halo, halo_sem.at[0])
    product[0:8, :] = jnp.where(ep == 0, 0.0, halo[...])
    top = 16
    mixed[0:top, :] = convolve(0, top)
    to_top = pl.multiple_of(((X - x) % X) * m_rows, m_rows)
    m_part[pl.ds(to_top, top), :] = jnp.dot(
        mixed[0:top, :], w_mix[...], preferred_element_type=F32
    ).astype(BF16)
    m_middle, m_end = rs_start(
        m_part, m_rows, [rel * m_rows for rel in range(X)], 0, m_turn, m_minus, m_plus, (0, D), MX, mx_sem, 0
    )

    with jax.named_scope("a_sent"):
        sent(send_a.at[pl.ds(CB, R - CB), cols_of(p.QA[0])], A)
    send_out(1)
    scoped("m_mid", m_middle)

    def where(j, rel):
        return pl.ds(p.off(j // GS, rel, j % GS), CB)

    def turn_in(q):
        c0, c1 = p.QA[q]
        cols = cols_of(p.QA[q])
        with jax.named_scope(f"a_wait#{q}"):
            arrived(recv_a.at[pl.ds(CB, R - CB), cols], a_sem.at[q])
        step = min(256, D // 8)

        def tile(i, _):
            part_cols = pl.ds(pl.multiple_of(c0 + i * step, step), step)
            moved = jnp.dot(perm[...], recv_a[0:R, part_cols], preferred_element_type=F32)
            moved = moved.astype(BF16)
            send_b[0:R, part_cols] = moved
            gathered[0:CB, part_cols] = moved[0:CB]
            return 0

        scoped(f"turn_in#{q}", lambda: lax.fori_loop(0, (c1 - c0) // step, tile, 0))
        for j in p.sends[q]:
            start(
                send_b.at[pl.ds(j * CB, CB), cols], gathered.at[where(j, 0), cols],
                B, b_sem.at[q * NZ + j], line[j],
            )

    def gather_out(q, j):
        cols = cols_of(p.QA[q])
        i = 2 * (q * NZ + j)
        own = gathered.at[where(j, 0), cols]
        if j:
            arrived(own, b_sem.at[q * NZ + j])
        start(own, gathered.at[where(j, 3), cols], AG, ag_sem.at[i], right)
        start(own, gathered.at[where(j, 1), cols], AG, ag_sem.at[i + 1], left)

    def gather_on(q, j):
        c0, c1 = p.QA[q]
        mid = (c0 + c1) // 2
        cols, lo, hi = cols_of(p.QA[q]), pl.ds(c0, mid - c0), pl.ds(mid, c1 - mid)
        i = 2 * (q * NZ + j)
        k = j // GS
        arrived(gathered.at[where(j, 3), cols], ag_sem.at[i])
        start(gathered.at[where(j, 3), lo], gathered.at[where(j, 2), lo], FW, fw_sem.at[k], right)
        arrived(gathered.at[where(j, 1), cols], ag_sem.at[i + 1])
        start(gathered.at[where(j, 1), hi], gathered.at[where(j, 2), hi], FW, fw_sem.at[k], left)

    rows_k = X * GS * CB

    def pieces(k):
        r0 = p.off(k, 0)

        def up(t, _):
            cols = pl.ds(pl.multiple_of(t * 128, 128), 128)
            pair = jnp.concatenate([w_gate[:, cols], w_up[:, cols]], axis=1)
            both = jnp.dot(gathered[r0 : r0 + rows_k, :], pair, preferred_element_type=F32)
            hid[:, cols] = (jax.nn.silu(both[:, :128]) * both[:, 128:]).astype(BF16)
            return 0

        def down(n, _):
            cols = pl.ds(pl.multiple_of(n * (D // 2), 128), D // 2)
            out = jnp.dot(hid[...], w_down[:, cols], preferred_element_type=F32).astype(BF16)
            for rel in range(X):
                to = rel * R + k * GS * CB
                part[to : to + GS * CB, cols] = out[rel * GS * CB : (rel + 1) * GS * CB]
            return 0

        def first():
            with jax.named_scope(f"cwait#{k}"):
                arrived(gathered.at[pl.ds(p.off(k, 2), GS * CB), :], fw_sem.at[k])
                if k == 0:
                    for copy in loads[1:]:
                        copy.wait()
            loop(up, 0, cuts[1])

        def loop(f, lo, hi):
            with jax.named_scope(f"{f.__name__}#{k},{lo}"):
                lax.fori_loop(lo, hi, f, 0)

        tiles, outs = F // 128, 2
        cuts = [0, (tiles + 2) // 3, (2 * tiles + 2) // 3, tiles]
        yield first
        yield lambda: loop(up, cuts[1], cuts[2])
        yield lambda: loop(up, cuts[2], cuts[3])
        yield lambda: loop(down, 0, (outs + 1) // 2)
        yield lambda: loop(down, (outs + 1) // 2, outs)

    rs = {}
    half = NZ // 2
    far_units = [(k * GS, GS, span) for span in p.QF for k in range(NG - 1, NG // 2 - 1, -1)]
    units = far_units + [(0, half, span) for span in p.QR]
    units = units[:2] + units[4:5] + units[2:4] + units[5:]

    def sum_start(n):
        j, count, span = units[n]
        rs[n] = rs_start(
            part, count * CB, [rel * R + j * CB for rel in range(X)], j * CB,
            turn, s_minus, s_plus, span, RS, rs_sem, 4 * n,
        )

    def back_sem(n):
        span = units[n][2]
        return rb_sem.at[p.QF.index(span)] if units[n][0] else rb_sem.at[len(p.QF) + p.QR.index(span)]

    def sum_end(n):
        j0, count, span = units[n]
        total = rs[n][1]()
        cols = cols_of(span)
        out_b[j0 * CB : (j0 + count) * CB, cols] = total
        if j0 == 0:
            ret_b[0:CB, cols] = total[0:CB]
        for j in reversed(range(max(j0, 1), j0 + count)):
            rows = pl.ds(j * CB, CB)
            start(out_b.at[rows, cols], ret_b.at[rows, cols], RB, back_sem(n), line_back[j])

    far_back = set()
    slot_j = lax.broadcasted_iota(jnp.int32, (T, R), 1)
    w_cols = [as_col(route_weights[k : k + 1, :]) for k in range(2)]
    mix = jnp.where(slot_j == slots[0], w_cols[0], 0.0)
    mix = mix + jnp.where(slot_j == slots[1], w_cols[1], 0.0)
    mix_hi[...] = mix.astype(BF16)
    mix_lo[...] = (mix - mix_hi[...].astype(F32)).astype(BF16)

    def turn_out(q):
        cols = cols_of(p.QR[q])
        with jax.named_scope(f"rb_wait#{q}"):
            for i, span in enumerate(p.QF):
                if span[0] < p.QR[q][1] and i not in far_back:
                    far_back.add(i)
                    arrived(ret_b.at[pl.ds(half * CB, R - half * CB), cols_of(span)], rb_sem.at[i])
            arrived(ret_b.at[pl.ds(CB, (half - 1) * CB), cols], rb_sem.at[len(p.QF) + q])
        with jax.named_scope(f"turn_out#{q}"):
            moved = jnp.dot(perm[...], ret_b[0:R, cols], preferred_element_type=F32).astype(BF16)
            send_r[0:R, cols] = moved
            ret_a[0:CB, cols] = moved[0:CB]
        for d in range(1, G):
            rows = pl.ds(d * CB, CB)
            start(send_r.at[rows, cols], ret_a.at[rows, cols], RA, ra_sem.at[q], plane_back[d])

    def combine(q):
        cols = cols_of(p.QR[q])
        with jax.named_scope(f"ra_wait#{q}"):
            arrived(ret_a.at[pl.ds(CB, R - CB), cols], ra_sem.at[q])
        with jax.named_scope(f"combine#{q}"):
            rows = ret_a[0:R, cols]
            total = jnp.dot(mix_hi[...], rows, preferred_element_type=F32)
            total = total + jnp.dot(mix_lo[...], rows, preferred_element_type=F32)
            moe_out[:, cols] = total.astype(BF16)

    work, computed = [], set()

    def do_work(count):
        while count and work:
            k, n, piece = work.pop(0)
            piece()
            count -= 1
            if n == 4:
                computed.add(k)

    script = (
        "t0 o00 o01 n00",
        "o02 n01 o03 n02",
        "o04 t1 n03 o10",
        "o06 o07 n04 o05",
        "n10 o11 o12 n06",
        "n07 n05 n11 o17",
        "o16 n12 w0 c1",
        "n17 o15 c1 n16",
        "c2 o14 o13 c1",
        "n15 w3 c1 n14",
        "c2 n13 c2 s0",
        "m w2 c3 i0",
        "c2 s1 w1 c3",
        "i1 c2 s2",
    )
    for event in itertools.chain(*(line.split() for line in script)):
        kind, at_n = event[0], [int(digit) for digit in event[1:]]
        if kind == "t":
            turn_in(*at_n)
        elif kind == "o":
            scoped("gout#" + event, gather_out, *at_n)
        elif kind == "n":
            scoped("gon#" + event, gather_on, *at_n)
        elif kind == "w":
            work.extend((at_n[0], n, piece) for n, piece in enumerate(pieces(at_n[0])))
        elif kind == "c":
            do_work(*at_n)
        elif kind == "s":
            scoped("sstart#" + event, sum_start, *at_n)
        elif kind == "i":
            scoped("smid#" + event, rs[at_n[0]][0])
        elif kind == "m":
            with jax.named_scope("m_end"):
                mixer_out[...] = m_end()
    last, turns = len(p.QR) - 1, {4: 0}
    begun = 3
    for n in range(len(units) + 1):
        while begun < len(units) and begun <= n + 2:
            scoped(f"sstart#{begun}", sum_start, begun)
            begun += 1
        if 2 <= n < len(units):
            scoped(f"smid#{n}", rs[n][0])
        if n >= 1:
            scoped(f"send#{n - 1}", sum_end, n - 1)
        if n - 1 in turns:
            turn_out(turns[n - 1])
    turn_out(1)
    turn_out(2)
    turn_out(last)
    for q in range(last + 1):
        combine(q)
    with jax.named_scope("sends"):
        sent(halo, HALO)
        sent(send_a.at[pl.ds(CB, R - CB), cols_of(p.QA[1])], A + 9)
        sent(send_b.at[pl.ds(CB, R - CB), :], B)
        sent(gathered.at[pl.ds(0, 2 * R), :], AG)
        sent(gathered.at[pl.ds(0, R), :], FW)
        sent(part.at[pl.ds(0, 3 * R), :], RS)
        sent(m_part.at[pl.ds(0, 3 * m_rows), :], MX)
        sent(out_b.at[pl.ds(CB, R - CB), :], RB)
        sent(send_r.at[pl.ds(CB, R - CB), :], RA)


def hand_over(*refs):
    count = len(refs) // 2
    for source, target in zip(refs[:count], refs[count:]):
        target[...] = source[...]


def permutation(p):
    matrix = np.zeros((p.R, p.R), np.float32)
    for j in range(p.NZ):
        for d in range(p.G):
            for r in range(CAP):
                matrix[j * p.CB + d * CAP + r, d * p.CB + j * CAP + r] = 1.0
    return jnp.asarray(matrix, BF16)


def on_device(
    c_gate, b_gate, values, conv_taps, w_mix_out, moe_in, norm_gain,
    route_ids, route_weights, w_gate, w_up, w_down,
):
    n_ep, n_tp = lax.axis_size("ep"), lax.axis_size("tp")
    p = Plan(n_ep, n_tp, moe_in.shape[1], w_gate.shape[2], moe_in.shape[0], *c_gate.shape)
    D, F, T, R, CB, G, NZ, X = p.D, p.F, p.T, p.R, p.CB, p.G, p.NZ, p.X
    m_rows = p.TA // X
    vmem = pl.BlockSpec(memory_space=pltpu.VMEM)
    hbm = pl.BlockSpec(memory_space=pl.ANY)
    block = pltpu.VMEM((R + PAD, D), BF16)
    dma = pltpu.SemaphoreType.DMA
    outs = pl.pallas_call(
        functools.partial(body, p),
        name="mixer_and_experts",
        out_shape=(
            jax.ShapeDtypeStruct((m_rows, D), BF16),
            jax.ShapeDtypeStruct((T, D), BF16),
        ),
        in_specs=[vmem, vmem, vmem, vmem, hbm, vmem, vmem, vmem, vmem, vmem, hbm, hbm, hbm],
        out_specs=(vmem, vmem),
        scratch_shapes=[
            pltpu.VMEM(w_mix_out.shape, BF16),
            pltpu.VMEM((D, F), BF16),
            pltpu.VMEM((D, F), BF16),
            pltpu.VMEM((F, D), BF16),
            pltpu.VMEM((p.TA + 8, p.C), F32),
            pltpu.VMEM((8, p.C), F32),
            pltpu.VMEM((p.TA, p.C), BF16),
            pltpu.VMEM((p.TA, D), BF16),
            pltpu.VMEM((m_rows, D), BF16),
            pltpu.VMEM((m_rows, D), BF16),
            pltpu.VMEM((m_rows, D), BF16),
            pltpu.VMEM((T, D), BF16),
            block,
            block,
            block,
            pltpu.VMEM((X * R + PAD, D), BF16),
            pltpu.VMEM((X * p.GS * CB, F), BF16),
            pltpu.VMEM((X * R + PAD, D), BF16),
            block,
            block,
            block,
            block,
            block,
            block,
            block,
            pltpu.VMEM((T, R), BF16),
            pltpu.VMEM((T, R), BF16),
            dma((4,)),
            dma((11,)),
            dma((1,)),
            dma((len(p.QA),)),
            dma((len(p.QA) * NZ,)),
            dma((len(p.QA) * 2 * NZ,)),
            dma((p.NG,)),
            dma((4 * (p.NG // 2 * len(p.QF) + len(p.QR)),)),
            dma((4,)),
            dma((len(p.QF) + len(p.QR),)),
            dma((len(p.QR),)),
        ],
        compiler_params=pltpu.CompilerParams(
            collective_id=0, has_side_effects=True, vmem_limit_bytes=60 * 2**20
        ),
    )(
        c_gate, b_gate, values, conv_taps, w_mix_out, moe_in, norm_gain.reshape(1, -1),
        route_ids.T, route_weights.T, permutation(p), w_gate, w_up, w_down,
    )
    return pl.pallas_call(
        hand_over,
        name="hand_over",
        out_shape=tuple(jax.ShapeDtypeStruct(out.shape, out.dtype) for out in outs),
        in_specs=[vmem] * len(outs),
        out_specs=tuple([vmem] * len(outs)),
    )(*outs)


def solution(mesh):
    return jax.shard_map(
        on_device,
        mesh=mesh,
        in_specs=(
            P("ep", "tp"),
            P("ep", "tp"),
            P("ep", "tp"),
            P(None, "tp"),
            P("tp", None),
            P(("ep", "tp"), None),
            P(),
            P(("ep", "tp"), None),
            P(("ep", "tp"), None),
            P("ep", None, "tp"),
            P("ep", None, "tp"),
            P("ep", "tp", None),
        ),
        out_specs=(P(("ep", "tp"), None), P(("ep", "tp"), None)),
        check_vma=False,
    )
```

```python
import functools
import itertools

import jax
import jax.numpy as jnp
import numpy as np
from jax import lax
from jax.experimental import pallas as pl
from jax.experimental.pallas import tpu as pltpu
from jax.sharding import PartitionSpec as P

EPS = 1e-06
MESH = pl.DeviceIdType.MESH
F32 = jnp.float32
BF16 = jnp.bfloat16
CAP = 5
PAD = 8


class Plan:
    def __init__(self, n_ep, n_tp, width, hidden, rows, tokens, channels):
        self.G = int(round(n_ep**0.5))
        self.NZ = n_ep // self.G
        assert self.G * self.NZ == n_ep and self.G == self.NZ and n_tp == 4
        self.X = n_tp
        self.D, self.F, self.T = width, hidden, rows
        self.TA, self.C = tokens, channels
        self.CB = CAP * self.G
        self.R = self.CB * self.NZ
        self.GS = 2
        self.NG = self.NZ // self.GS
        far = self.NZ // 2
        self.dz = [0]
        for step in range(1, far - 1):
            self.dz += [-step, step]
        self.dz += [far, 1 - far, far - 1]
        assert len(self.dz) == self.NZ
        near_first = sorted(range(1, self.NZ), key=lambda j: abs(self.dz[j]))
        self.sends = [near_first, [1, 2] + list(range(self.NZ - 1, 2, -1))]
        eighth = width // 8
        self.QA = spans([3 * eighth, 5 * eighth])
        self.QR = spans([4 * eighth, 2 * eighth, eighth, eighth])
        self.QF = spans([6 * eighth, 2 * eighth])
        assert self.NZ == 8

    def off(self, k, rel, jj=0):
        return ((k * self.X + rel) * self.GS + jj) * self.CB


def spans(widths):
    ends = list(itertools.accumulate(widths))
    return [(end - width, end) for width, end in zip(widths, ends)]


def scoped(name, f, *a):
    with jax.named_scope(name):
        return f(*a)


def body(
    p,
    c_gate,
    b_gate,
    values,
    conv_taps,
    w_mix_hbm,
    moe_in,
    norm_gain,
    route_ids,
    route_weights,
    perm,
    w_gate_hbm,
    w_up_hbm,
    w_down_hbm,
    mixer_out,
    moe_out,
    w_mix,
    w_gate,
    w_up,
    w_down,
    product,
    halo,
    mixed,
    m_part,
    m_turn,
    m_minus,
    m_plus,
    normed,
    send_a,
    recv_a,
    send_b,
    gathered,
    hid,
    part,
    turn,
    s_minus,
    s_plus,
    out_b,
    ret_b,
    send_r,
    ret_a,
    mix_hi,
    mix_lo,
    w_sem,
    send_sem,
    halo_sem,
    a_sem,
    b_sem,
    ag_sem,
    fw_sem,
    rs_sem,
    mx_sem,
    rb_sem,
    ra_sem,
):
    G, NZ, X, D, F, T, CB, R, GS, NG = p.G, p.NZ, p.X, p.D, p.F, p.T, p.CB, p.R, p.GS, p.NG
    ep, x = lax.axis_index("ep"), lax.axis_index("tp")
    z, g = ep // G, ep % G

    def at(zz, gg, xx):
        return {"ep": zz * G + gg, "tp": xx}

    right, left = at(z, g, (x + 1) % X), at(z, g, (x + X - 1) % X)
    after = {"ep": (ep + 1) % (G * NZ), "tp": x}
    before = {"ep": (ep + G * NZ - 1) % (G * NZ), "tp": x}
    plane = [at(z, (g + d) % G, x) for d in range(G)]
    plane_back = [at(z, (g + G - d) % G, x) for d in range(G)]
    line = [at((z + NZ + dz) % NZ, g, x) for dz in p.dz]
    line_back = [at((z + NZ - dz) % NZ, g, x) for dz in p.dz]

    barrier = pltpu.get_barrier_semaphore()
    peers = plane[1:] + line[1:] + [right, left, after, before]
    for peer in peers:
        pl.semaphore_signal(barrier, inc=1, device_id=peer, device_id_type=MESH)

    def load(src, dst, i):
        copy = pltpu.make_async_copy(src, dst, w_sem.at[i])
        copy.start()
        return copy

    loads = [
        load(w_mix_hbm, w_mix, 0),
        load(w_gate_hbm.at[0], w_gate, 1),
        load(w_up_hbm.at[0], w_up, 2),
        load(w_down_hbm.at[0], w_down, 3),
    ]
    def start(src, dst, send, recv, peer):
        copy = pltpu.make_async_remote_copy(
            src_ref=src,
            dst_ref=dst,
            send_sem=send_sem.at[send],
            recv_sem=recv,
            device_id=peer,
            device_id_type=MESH,
        )
        copy.start()
        return copy

    def arrived(ref, recv):
        pltpu.make_async_remote_copy(
            src_ref=ref, dst_ref=ref, send_sem=send_sem.at[0], recv_sem=recv,
            device_id=right, device_id_type=MESH,
        ).wait_recv()

    def sent(ref, send):
        pltpu.make_async_remote_copy(
            src_ref=ref, dst_ref=ref, send_sem=send_sem.at[send], recv_sem=halo_sem.at[0],
            device_id=right, device_id_type=MESH,
        ).wait_send()

    HALO, A, B, AG, FW, RS, MX, RB, RA = range(9)

    tokens = p.TA
    product[8 : 8 + tokens, :] = c_gate[...].astype(F32) * values[...].astype(F32)

    stream = moe_in[...].astype(F32)
    scale = lax.rsqrt(jnp.mean(stream * stream, axis=1, keepdims=True) + EPS)
    normed[...] = (stream * scale * norm_gain[...]).astype(BF16)

    rows_i = lax.broadcasted_iota(jnp.int32, (T, T), 0)
    cols_i = lax.broadcasted_iota(jnp.int32, (T, T), 1)
    eye, earlier = rows_i == cols_i, cols_i < rows_i

    def as_row(col):
        return jnp.sum(jnp.where(eye, col, 0.0), axis=0, keepdims=True)

    def as_col(row):
        return jnp.sum(jnp.where(eye, row, 0.0), axis=1, keepdims=True)

    id_rows = [route_ids[k : k + 1, :].astype(F32) for k in range(2)]
    slots = []
    for col in [as_col(row) for row in id_rows]:
        seen = jnp.zeros((T, 1), F32)
        for row in id_rows:
            seen = seen + jnp.sum(
                jnp.where(earlier & (col == row), 1.0, 0.0), axis=1, keepdims=True
            )
        rank, expert = seen.astype(jnp.int32), col.astype(jnp.int32)
        to_g = (expert & (G - 1)) - g
        to_g = jnp.where(to_g < 0, to_g + G, to_g)
        to_z = (expert >> (G.bit_length() - 1)) - z
        to_z = jnp.where(to_z < 0, to_z + NZ, to_z)
        slot_z = jnp.zeros_like(to_z)
        for j, dz in enumerate(p.dz):
            slot_z = jnp.where(to_z == dz % NZ, j, slot_z)
        slots.append(to_g * CB + slot_z * CAP + rank)
    slot_rows = [as_row(col.astype(F32)).astype(jnp.int32) for col in slots]
    slot_i = lax.broadcasted_iota(jnp.int32, (R, T), 0)
    pick = jnp.where((slot_i == slot_rows[0]) | (slot_i == slot_rows[1]), 1.0, 0.0).astype(BF16)
    wide = min(512, D)

    def pack(i, _):
        cols = pl.ds(pl.multiple_of(i * wide, wide), wide)
        packed = jnp.dot(pick, normed[:, cols], preferred_element_type=F32).astype(BF16)
        send_a[0:R, cols] = packed
        recv_a[0:CB, cols] = packed[0:CB]
        return 0

    scoped("pack", lambda: lax.fori_loop(0, D // wide, pack, 0))

    scoped("barrier", pl.semaphore_wait, barrier, len(peers))

    start(product.at[pl.ds(tokens, 8)], halo, HALO, halo_sem.at[0], after)

    def cols_of(span):
        return pl.ds(span[0], span[1] - span[0])

    def send_out(q):
        cols = cols_of(p.QA[q])
        for d in range(1, G):
            rows = pl.ds(d * CB, CB)
            start(send_a.at[rows, cols], recv_a.at[rows, cols], A + 9 * q, a_sem.at[q], plane[d])

    send_out(0)

    def rs_start(src, rows, offs, dst_off, turn, minus, plus, span, send, sems, i):
        c0, c1 = span
        mid = (c0 + c1) // 2
        lo, hi = pl.ds(c0, mid - c0), pl.ds(mid, c1 - mid)
        cols = cols_of(span)
        o0, o1, o2, o3 = (pl.ds(o, rows) for o in offs)
        od = pl.ds(dst_off, rows)
        turn_lo, turn_hi, from_minus, from_plus = (sems.at[i + n] for n in range(4))
        start(src.at[o2, lo], turn.at[od, lo], send, turn_lo, right)
        start(src.at[o2, hi], turn.at[od, hi], send, turn_hi, left)
        start(src.at[o1, hi], minus.at[od, hi], send, from_minus, right)
        start(src.at[o3, lo], plus.at[od, lo], send, from_plus, left)

        def middle():
            arrived(turn.at[od, lo], turn_lo)
            src[o1, lo] = (src[o1, lo].astype(F32) + turn[od, lo].astype(F32)).astype(BF16)
            start(src.at[o1, lo], minus.at[od, lo], send, from_minus, right)
            arrived(turn.at[od, hi], turn_hi)
            src[o3, hi] = (src[o3, hi].astype(F32) + turn[od, hi].astype(F32)).astype(BF16)
            start(src.at[o3, hi], plus.at[od, hi], send, from_plus, left)

        def end():
            arrived(minus.at[od, cols], from_minus)
            arrived(plus.at[od, cols], from_plus)
            total = src[o0, cols].astype(F32) + minus[od, cols].astype(F32)
            return (total + plus[od, cols].astype(F32)).astype(BF16)

        return middle, end

    def convolve(first, count):
        taps = conv_taps.shape[0]
        convolved = jnp.zeros((count, p.C), F32)
        for k in range(taps):
            reach = product[8 - taps + 1 + k + first : 8 - taps + 1 + k + first + count, :]
            convolved = convolved + conv_taps[k : k + 1, :] * reach
        return (b_gate[first : first + count, :].astype(F32) * convolved).astype(BF16)

    product[0:8, :] = jnp.zeros((8, p.C), F32)
    mixed[...] = convolve(0, tokens)
    scoped("wmix", loads[0].wait)
    m_rows = tokens // X
    for rel in range(X):
        own = pl.ds(pl.multiple_of(((x + rel) % X) * m_rows, m_rows), m_rows)
        m_part[pl.ds(rel * m_rows, m_rows), :] = jnp.dot(
            mixed[own, :], w_mix[...], preferred_element_type=F32
        ).astype(BF16)
    scoped("halo", arrived, halo, halo_sem.at[0])
    product[0:8, :] = jnp.where(ep == 0, 0.0, halo[...])
    top = 16
    mixed[0:top, :] = convolve(0, top)
    to_top = pl.multiple_of(((X - x) % X) * m_rows, m_rows)
    m_part[pl.ds(to_top, top), :] = jnp.dot(
        mixed[0:top, :], w_mix[...], preferred_element_type=F32
    ).astype(BF16)
    m_middle, m_end = rs_start(
        m_part, m_rows, [rel * m_rows for rel in range(X)], 0, m_turn, m_minus, m_plus, (0, D), MX, mx_sem, 0
    )

    with jax.named_scope("a_sent"):
        sent(send_a.at[pl.ds(CB, R - CB), cols_of(p.QA[0])], A)
    send_out(1)
    scoped("m_mid", m_middle)

    def where(j, rel):
        return pl.ds(p.off(j // GS, rel, j % GS), CB)

    def turn_in(q):
        c0, c1 = p.QA[q]
        cols = cols_of(p.QA[q])
        with jax.named_scope(f"a_wait#{q}"):
            arrived(recv_a.at[pl.ds(CB, R - CB), cols], a_sem.at[q])
        step = min(256, D // 8)

        def tile(i, _):
            part_cols = pl.ds(pl.multiple_of(c0 + i * step, step), step)
            moved = jnp.dot(perm[...], recv_a[0:R, part_cols], preferred_element_type=F32)
            moved = moved.astype(BF16)
            send_b[0:R, part_cols] = moved
            gathered[0:CB, part_cols] = moved[0:CB]
            return 0

        scoped(f"turn_in#{q}", lambda: lax.fori_loop(0, (c1 - c0) // step, tile, 0))
        for j in p.sends[q]:
            start(
                send_b.at[pl.ds(j * CB, CB), cols], gathered.at[where(j, 0), cols],
                B, b_sem.at[q * NZ + j], line[j],
            )

    def gather_out(q, j):
        cols = cols_of(p.QA[q])
        i = 2 * (q * NZ + j)
        own = gathered.at[where(j, 0), cols]
        if j:
            arrived(own, b_sem.at[q * NZ + j])
        start(own, gathered.at[where(j, 3), cols], AG, ag_sem.at[i], right)
        start(own, gathered.at[where(j, 1), cols], AG, ag_sem.at[i + 1], left)

    def gather_on(q, j):
        c0, c1 = p.QA[q]
        mid = (c0 + c1) // 2
        cols, lo, hi = cols_of(p.QA[q]), pl.ds(c0, mid - c0), pl.ds(mid, c1 - mid)
        i = 2 * (q * NZ + j)
        k = j // GS
        arrived(gathered.at[where(j, 3), cols], ag_sem.at[i])
        start(gathered.at[where(j, 3), lo], gathered.at[where(j, 2), lo], FW, fw_sem.at[k], right)
        arrived(gathered.at[where(j, 1), cols], ag_sem.at[i + 1])
        start(gathered.at[where(j, 1), hi], gathered.at[where(j, 2), hi], FW, fw_sem.at[k], left)

    rows_k = X * GS * CB

    def pieces(k):
        r0 = p.off(k, 0)

        def up(t, _):
            cols = pl.ds(pl.multiple_of(t * 128, 128), 128)
            pair = jnp.concatenate([w_gate[:, cols], w_up[:, cols]], axis=1)
            both = jnp.dot(gathered[r0 : r0 + rows_k, :], pair, preferred_element_type=F32)
            hid[:, cols] = (jax.nn.silu(both[:, :128]) * both[:, 128:]).astype(BF16)
            return 0

        def down(n, _):
            cols = pl.ds(pl.multiple_of(n * (D // 2), 128), D // 2)
            out = jnp.dot(hid[...], w_down[:, cols], preferred_element_type=F32).astype(BF16)
            for rel in range(X):
                to = rel * R + k * GS * CB
                part[to : to + GS * CB, cols] = out[rel * GS * CB : (rel + 1) * GS * CB]
            return 0

        def first():
            with jax.named_scope(f"cwait#{k}"):
                arrived(gathered.at[pl.ds(p.off(k, 2), GS * CB), :], fw_sem.at[k])
                if k == 0:
                    for copy in loads[1:]:
                        copy.wait()
            loop(up, 0, cuts[1])

        def loop(f, lo, hi):
            with jax.named_scope(f"{f.__name__}#{k},{lo}"):
                lax.fori_loop(lo, hi, f, 0)

        tiles, outs = F // 128, 2
        cuts = [0, (tiles + 2) // 3, (2 * tiles + 2) // 3, tiles]
        yield first
        yield lambda: loop(up, cuts[1], cuts[2])
        yield lambda: loop(up, cuts[2], cuts[3])
        yield lambda: loop(down, 0, (outs + 1) // 2)
        yield lambda: loop(down, (outs + 1) // 2, outs)

    rs = {}
    half = NZ // 2
    far_units = [(k * GS, GS, span) for span in p.QF for k in range(NG - 1, NG // 2 - 1, -1)]
    units = far_units + [(0, half, span) for span in p.QR]
    units = units[:2] + units[4:5] + units[2:4] + units[5:]

    def sum_start(n):
        j, count, span = units[n]
        rs[n] = rs_start(
            part, count * CB, [rel * R + j * CB for rel in range(X)], j * CB,
            turn, s_minus, s_plus, span, RS, rs_sem, 4 * n,
        )

    def back_sem(n):
        span = units[n][2]
        return rb_sem.at[p.QF.index(span)] if units[n][0] else rb_sem.at[len(p.QF) + p.QR.index(span)]

    def sum_end(n):
        j0, count, span = units[n]
        total = rs[n][1]()
        cols = cols_of(span)
        out_b[j0 * CB : (j0 + count) * CB, cols] = total
        if j0 == 0:
            ret_b[0:CB, cols] = total[0:CB]
        for j in reversed(range(max(j0, 1), j0 + count)):
            rows = pl.ds(j * CB, CB)
            start(out_b.at[rows, cols], ret_b.at[rows, cols], RB, back_sem(n), line_back[j])

    far_back = set()
    slot_j = lax.broadcasted_iota(jnp.int32, (T, R), 1)
    w_cols = [as_col(route_weights[k : k + 1, :]) for k in range(2)]
    mix = jnp.where(slot_j == slots[0], w_cols[0], 0.0)
    mix = mix + jnp.where(slot_j == slots[1], w_cols[1], 0.0)
    mix_hi[...] = mix.astype(BF16)
    mix_lo[...] = (mix - mix_hi[...].astype(F32)).astype(BF16)

    def turn_out(q):
        cols = cols_of(p.QR[q])
        with jax.named_scope(f"rb_wait#{q}"):
            for i, span in enumerate(p.QF):
                if span[0] < p.QR[q][1] and i not in far_back:
                    far_back.add(i)
                    arrived(ret_b.at[pl.ds(half * CB, R - half * CB), cols_of(span)], rb_sem.at[i])
            arrived(ret_b.at[pl.ds(CB, (half - 1) * CB), cols], rb_sem.at[len(p.QF) + q])
        with jax.named_scope(f"turn_out#{q}"):
            moved = jnp.dot(perm[...], ret_b[0:R, cols], preferred_element_type=F32).astype(BF16)
            send_r[0:R, cols] = moved
            ret_a[0:CB, cols] = moved[0:CB]
        for d in range(1, G):
            rows = pl.ds(d * CB, CB)
            start(send_r.at[rows, cols], ret_a.at[rows, cols], RA, ra_sem.at[q], plane_back[d])

    def combine(q):
        cols = cols_of(p.QR[q])
        with jax.named_scope(f"ra_wait#{q}"):
            arrived(ret_a.at[pl.ds(CB, R - CB), cols], ra_sem.at[q])
        with jax.named_scope(f"combine#{q}"):
            rows = ret_a[0:R, cols]
            total = jnp.dot(mix_hi[...], rows, preferred_element_type=F32)
            total = total + jnp.dot(mix_lo[...], rows, preferred_element_type=F32)
            moe_out[:, cols] = total.astype(BF16)

    work, computed = [], set()

    def do_work(count):
        while count and work:
            k, n, piece = work.pop(0)
            piece()
            count -= 1
            if n == 4:
                computed.add(k)

    script = (
        "t0 o00 o01 n00",
        "o02 n01 o03 n02",
        "o04 t1 n03 o10",
        "o06 o07 n04 o05",
        "n10 o11 o12 n06",
        "n07 n05 n11 o17",
        "o16 n12 w0 c1",
        "n17 o15 c1 n16",
        "c2 o14 o13 c1",
        "n15 w3 c1 n14",
        "c2 n13 c2 s0",
        "m w2 c3 i0",
        "c2 s1 w1 c3",
        "s3 i1 c2 s2",
    )
    for event in itertools.chain(*(line.split() for line in script)):
        kind, at_n = event[0], [int(digit) for digit in event[1:]]
        if kind == "t":
            turn_in(*at_n)
        elif kind == "o":
            scoped("gout#" + event, gather_out, *at_n)
        elif kind == "n":
            scoped("gon#" + event, gather_on, *at_n)
        elif kind == "w":
            work.extend((at_n[0], n, piece) for n, piece in enumerate(pieces(at_n[0])))
        elif kind == "c":
            do_work(*at_n)
        elif kind == "s":
            scoped("sstart#" + event, sum_start, *at_n)
        elif kind == "i":
            scoped("smid#" + event, rs[at_n[0]][0])
        elif kind == "m":
            with jax.named_scope("m_end"):
                mixer_out[...] = m_end()
    last, turns = len(p.QR) - 1, {4: 0}
    begun = 4
    for n in range(len(units) + 1):
        while begun < len(units) and begun <= n + 2:
            scoped(f"sstart#{begun}", sum_start, begun)
            begun += 1
        if 2 <= n < len(units):
            scoped(f"smid#{n}", rs[n][0])
        if n >= 1:
            scoped(f"send#{n - 1}", sum_end, n - 1)
        if n - 1 in turns:
            turn_out(turns[n - 1])
    turn_out(1)
    turn_out(2)
    turn_out(last)
    for q in range(last + 1):
        combine(q)
    with jax.named_scope("sends"):
        sent(halo, HALO)
        sent(send_a.at[pl.ds(CB, R - CB), cols_of(p.QA[1])], A + 9)
        sent(send_b.at[pl.ds(CB, R - CB), :], B)
        sent(gathered.at[pl.ds(0, 2 * R), :], AG)
        sent(gathered.at[pl.ds(0, R), :], FW)
        sent(part.at[pl.ds(0, 3 * R), :], RS)
        sent(m_part.at[pl.ds(0, 3 * m_rows), :], MX)
        sent(out_b.at[pl.ds(CB, R - CB), :], RB)
        sent(send_r.at[pl.ds(CB, R - CB), :], RA)


def hand_over(*refs):
    count = len(refs) // 2
    for source, target in zip(refs[:count], refs[count:]):
        target[...] = source[...]


def permutation(p):
    matrix = np.zeros((p.R, p.R), np.float32)
    for j in range(p.NZ):
        for d in range(p.G):
            for r in range(CAP):
                matrix[j * p.CB + d * CAP + r, d * p.CB + j * CAP + r] = 1.0
    return jnp.asarray(matrix, BF16)


def on_device(
    c_gate, b_gate, values, conv_taps, w_mix_out, moe_in, norm_gain,
    route_ids, route_weights, w_gate, w_up, w_down,
):
    n_ep, n_tp = lax.axis_size("ep"), lax.axis_size("tp")
    p = Plan(n_ep, n_tp, moe_in.shape[1], w_gate.shape[2], moe_in.shape[0], *c_gate.shape)
    D, F, T, R, CB, G, NZ, X = p.D, p.F, p.T, p.R, p.CB, p.G, p.NZ, p.X
    m_rows = p.TA // X
    vmem = pl.BlockSpec(memory_space=pltpu.VMEM)
    hbm = pl.BlockSpec(memory_space=pl.ANY)
    block = pltpu.VMEM((R + PAD, D), BF16)
    dma = pltpu.SemaphoreType.DMA
    outs = pl.pallas_call(
        functools.partial(body, p),
        name="mixer_and_experts",
        out_shape=(
            jax.ShapeDtypeStruct((m_rows, D), BF16),
            jax.ShapeDtypeStruct((T, D), BF16),
        ),
        in_specs=[vmem, vmem, vmem, vmem, hbm, vmem, vmem, vmem, vmem, vmem, hbm, hbm, hbm],
        out_specs=(vmem, vmem),
        scratch_shapes=[
            pltpu.VMEM(w_mix_out.shape, BF16),
            pltpu.VMEM((D, F), BF16),
            pltpu.VMEM((D, F), BF16),
            pltpu.VMEM((F, D), BF16),
            pltpu.VMEM((p.TA + 8, p.C), F32),
            pltpu.VMEM((8, p.C), F32),
            pltpu.VMEM((p.TA, p.C), BF16),
            pltpu.VMEM((p.TA, D), BF16),
            pltpu.VMEM((m_rows, D), BF16),
            pltpu.VMEM((m_rows, D), BF16),
            pltpu.VMEM((m_rows, D), BF16),
            pltpu.VMEM((T, D), BF16),
            block,
            block,
            block,
            pltpu.VMEM((X * R + PAD, D), BF16),
            pltpu.VMEM((X * p.GS * CB, F), BF16),
            pltpu.VMEM((X * R + PAD, D), BF16),
            block,
            block,
            block,
            block,
            block,
            block,
            block,
            pltpu.VMEM((T, R), BF16),
            pltpu.VMEM((T, R), BF16),
            dma((4,)),
            dma((11,)),
            dma((1,)),
            dma((len(p.QA),)),
            dma((len(p.QA) * NZ,)),
            dma((len(p.QA) * 2 * NZ,)),
            dma((p.NG,)),
            dma((4 * (p.NG // 2 * len(p.QF) + len(p.QR)),)),
            dma((4,)),
            dma((len(p.QF) + len(p.QR),)),
            dma((len(p.QR),)),
        ],
        compiler_params=pltpu.CompilerParams(
            collective_id=0, has_side_effects=True, vmem_limit_bytes=60 * 2**20
        ),
    )(
        c_gate, b_gate, values, conv_taps, w_mix_out, moe_in, norm_gain.reshape(1, -1),
        route_ids.T, route_weights.T, permutation(p), w_gate, w_up, w_down,
    )
    return pl.pallas_call(
        hand_over,
        name="hand_over",
        out_shape=tuple(jax.ShapeDtypeStruct(out.shape, out.dtype) for out in outs),
        in_specs=[vmem] * len(outs),
        out_specs=tuple([vmem] * len(outs)),
    )(*outs)


def solution(mesh):
    return jax.shard_map(
        on_device,
        mesh=mesh,
        in_specs=(
            P("ep", "tp"),
            P("ep", "tp"),
            P("ep", "tp"),
            P(None, "tp"),
            P("tp", None),
            P(("ep", "tp"), None),
            P(),
            P(("ep", "tp"), None),
            P(("ep", "tp"), None),
            P("ep", None, "tp"),
            P("ep", None, "tp"),
            P("ep", "tp", None),
        ),
        out_specs=(P(("ep", "tp"), None), P(("ep", "tp"), None)),
        check_vma=False,
    )
```
